512 devices in a mesh: ep: 32 (over z, x), tp: 16 (over y, core).
Axes of the slice: x: 4, y: 8, z: 8, core: 2. Of those that a mesh axis runs over, the one named last changes fastest.
Arguments:
- q_in: bfloat16 [16384, 1024], P('ep', 'tp'), may hold values from -6 to 6
- k_in: bfloat16 [16384, 256], P('ep'), may hold values from -6 to 6
- v_in: bfloat16 [16384, 256], P('ep'), may hold values from -6 to 6
- q_gain: float32 [64], replicated, may hold values from 0.1 to 1.9
- k_gain: float32 [64], replicated, may hold values from 0.1 to 1.9
- w_out: bfloat16 [1024, 2048], P('tp'), may hold values from -0.1875 to 0.1875
- post_gain: float32 [2048], replicated, may hold values from 0.1 to 1.9
- moe_in: bfloat16 [4096, 2048], P('ep'), may hold values from -6 to 6
- routes: int32 [4096, 2], P('ep'), may hold values from 0 to 31, all different within a row; in each aligned block of 128 rows (0 to 127, 128 to 255, ...) at most 12 rows name the same one
- route_logits: float32 [4096, 2], P('ep'), may hold values from -6 to 6
- pre_gain: float32 [2048], replicated, may hold values from 0.1 to 1.9
- w_gate: bfloat16 [32, 2048, 4096], P('ep', None, 'tp'), may hold values from -0.125 to 0.125
- w_up: bfloat16 [32, 2048, 4096], P('ep', None, 'tp'), may hold values from -0.125 to 0.125
- w_down: bfloat16 [32, 4096, 2048], P('ep', 'tp'), may hold values from -0.125 to 0.125
Outputs:
- attn_out: bfloat16 [16384, 2048], P(('ep', 'tp'))
- moe_out: bfloat16 [4096, 2048], P('ep', 'tp')
The draws below stay inside these ranges and needn't reach their ends.
Inputs may be any that keep to these rules, and one draw needn't show every extreme that they name: `routes`: each row names 2 different experts. Among the rows of one index of ep no expert is named by more than 12 rows, a bound that some block reaches of them.
All inputs are finite; a program needn't handle non-finite values.
Results may differ from the reference program's by a relative error of at most 0.018.
Values may be sent and summed in bfloat16 or wider, within the bound.
A program may use at most 64 MiB of HBM per device.

```python
import math
import jax
import jax.numpy as jnp
import numpy as np
from jax import lax

D = 2048
HEADS = 16
KV_HEADS = 4
HEAD = 64
GRID_W = 128
FFE = 4096
TOP = 2
TOKM_DEV = 128
SEQ = 16384
TOKM = 4096
EXPERTS = 32
HEADS_DEV = 1
FF_DEV = 256
CAP = 12
N_EP = 32
N_TP = 16


def strengthened(drawn, own_key, source, target, shards_of, factor):
    def block_of(axis_at):
        return (jnp.arange(drawn.shape[axis_at]) // (drawn.shape[axis_at] // shards_of)).reshape((-1,) + (1,) * (drawn.ndim - 1 - axis_at))

    one_side = jax.random.permutation(own_key, shards_of)[block_of(target)]
    far = (block_of(target) + shards_of // 2) % shards_of
    return jnp.where((block_of(source) == one_side) | (block_of(source) == far), factor * drawn, drawn)


def block_levels(key, extent, shards, low, largest):
    factor_of, own = 1.0, jax.random.fold_in(key, 6)
    for dim, shards_of in shards:
        heights = jnp.exp(jax.random.uniform(jax.random.fold_in(own, dim), (shards_of,), jnp.float32, low / len(shards), largest / len(shards)))
        factor_of = factor_of * jnp.repeat(heights, extent[dim] // shards_of).reshape([-1 if axis == dim else 1 for axis in range(len(extent))])
    return factor_of


def assign_block(own_key, own, number, rows, number_of, top, bound, slope):
    order = jax.random.permutation(own_key, number_of)
    heavy_load, usual = load_shares(number_of, rows * top, bound, slope, True), load_shares(number_of, rows * top, bound, slope, False)
    places = jnp.arange(number_of)

    def named(lengths, offset_by):
        used = int((lengths > 0).sum())
        fixed = max(1, used // 4)
        shifted = fixed + (places - fixed + offset_by * (used - fixed)) % max(1, number_of - fixed)
        return jnp.zeros((number_of,), jnp.int32).at[order[jnp.where(places < fixed, places, shifted)]].set(jnp.asarray(lengths, jnp.int32))

    lengths = jnp.where(number % 4 == 0, named(heavy_load, number // 4), named(usual, number - number // 4 - 1))
    mixed = jax.random.permutation(jax.random.fold_in(own, 3), number_of)
    source_of, taker = mixed[0:number_of // 2 * 2:2], mixed[1:number_of // 2 * 2:2]
    margin = jnp.minimum(lengths[source_of] - 1, bound - lengths[taker]) // 2
    margin = jnp.where((source_of == order[0]) | (taker == order[0]) | (lengths[taker] == 0), 0, jnp.maximum(margin, 0))
    shifted = jax.random.randint(jax.random.fold_in(own, 4), (number_of // 2,), 0, 1 << 20) % (margin + 1)
    lengths = lengths.at[source_of].add(-shifted).at[taker].add(shifted)
    labels = jnp.searchsorted(jnp.cumsum(lengths), jnp.arange(rows * top), side="right").astype(jnp.int32)
    grid = labels.reshape(top, rows).T
    grid = grid[jax.random.permutation(jax.random.fold_in(own, 1), rows)]
    offset_by = jax.random.randint(jax.random.fold_in(own, 2), (rows, 1), 0, top)
    return jnp.take_along_axis(grid, (jnp.arange(top)[None, :] + offset_by) % top, axis=1)


def load_shares(number_of, total, limit, slope, full):
    weights = [(1 << 20) // math.isqrt(rank ** slope) + 1 for rank in range(1, number_of + 1)]
    largest = limit if full else min(limit, max(-(-total // number_of), total * weights[0] // sum(weights)))
    least = 1 if total - largest >= number_of - 1 else 0
    given, surplus = [largest] + [least] * (number_of - 1), total - largest - least * (number_of - 1)
    while surplus > 0:
        movable = [i for i in range(1, number_of) if given[i] < largest] or [i for i in range(1, number_of) if given[i] < limit]
        pool, budget = sum([weights[i] for i in movable]), surplus
        for i in movable:
            extra = min(limit - given[i], max(1, budget * weights[i] // pool), surplus)
            given[i] = given[i] + extra
            surplus = surplus - extra
    return np.array(given)


def noise(stream_key, extent, deviation, reach, cuts=(), kind=jnp.bfloat16):
    drawn = deviation * jax.random.normal(stream_key, extent, jnp.float32)
    if cuts:
        drawn = drawn * block_levels(stream_key, extent, cuts, -0.22, 0.18)
    return jnp.clip(drawn, -reach, reach).astype(kind)


def heavy_noise(own_key, dims, deviation, most, pieces, heavy, held_as=jnp.bfloat16):
    result = deviation * jax.random.normal(own_key, dims, jnp.float32)
    if pieces:
        result = result * block_levels(own_key, dims, pieces, -0.22, 0.18)
    return jnp.clip(strengthened(result, jax.random.fold_in(own_key, 3), *heavy), -most, most).astype(held_as)


def setup_inputs(seed: int = 0) -> dict:
    arg_keys = jax.random.split(jax.random.key(seed), 15)
    q_in = noise(arg_keys[0], (SEQ, HEADS * HEAD), 1.0, 6.0, ((0, 32), (1, 16)))
    k_in = noise(arg_keys[1], (SEQ, KV_HEADS * HEAD), 1.0, 6.0, ((0, 32),))
    v_in = noise(arg_keys[2], (SEQ, KV_HEADS * HEAD), 1.0, 6.0, ((0, 32),))
    q_gain = jnp.clip(1.0 + 0.18 * jax.random.normal(arg_keys[3], (HEAD,), jnp.float32), 0.1, 1.9)
    k_gain = jnp.clip(1.0 + 0.18 * jax.random.normal(arg_keys[4], (HEAD,), jnp.float32), 0.1, 1.9)
    w_out = noise(arg_keys[5], (HEADS * HEAD, D), (HEADS * HEAD) ** -0.5, 0.1875, ((0, 16),))
    post_gain = jnp.clip(1.0 + 0.18 * jax.random.normal(arg_keys[6], (D,), jnp.float32), 0.1, 1.9)
    moe_in = noise(arg_keys[7], (TOKM, D), 1.0, 6.0, ((0, 32),))
    routes_keys = jax.random.split(jax.random.fold_in(arg_keys[8], 1), TOKM // TOKM_DEV)
    routes_turns = jax.random.permutation(jax.random.fold_in(arg_keys[8], 3), TOKM // TOKM_DEV)
    routes = jax.vmap(lambda own, number: assign_block(jax.random.fold_in(arg_keys[8], 2), own, number, TOKM_DEV, EXPERTS, TOP, CAP, 2))(routes_keys, routes_turns).reshape((TOKM, TOP))
    route_logits = noise(arg_keys[9], (TOKM, TOP), 1.5, 6.0, ((0, 32),), jnp.float32)
    pre_gain = jnp.clip(1.0 + 0.18 * jax.random.normal(arg_keys[10], (D,), jnp.float32), 0.1, 1.9)
    w_gate = noise(arg_keys[11], (EXPERTS, D, FFE), D ** -0.5, 0.125, ((0, 32), (2, 16)))
    w_up = noise(arg_keys[12], (EXPERTS, D, FFE), D ** -0.5, 0.125, ((0, 32), (2, 16)))
    w_down = heavy_noise(arg_keys[13], (EXPERTS, FFE, D), FFE ** -0.5, 0.125, ((0, 32), (1, 16)), (1, 2, 16, 2.0))
    return {"q_in": q_in, "k_in": k_in, "v_in": v_in, "q_gain": q_gain, "k_gain": k_gain, "w_out": w_out, "post_gain": post_gain, "moe_in": moe_in, "routes": routes, "route_logits": route_logits, "pre_gain": pre_gain, "w_gate": w_gate, "w_up": w_up, "w_down": w_down}


EPSILON = 1e-06
ROPE_BASE = 10000.0

def head_norm(values, gain):
    return values * lax.rsqrt(lax.optimization_barrier(jnp.mean(values * values, axis=-1, keepdims=True)) + EPSILON) * gain

def rotate_half(values, angles):
    quarter = angles.shape[-1]
    first_part = values[..., :quarter]
    second_part = values[..., quarter:]
    cosine = jnp.cos(angles)[:, None, :]
    sine_part = jnp.sin(angles)[:, None, :]
    return jnp.concatenate([first_part * cosine - second_part * sine_part, second_part * cosine + first_part * sine_part], axis=-1)

def grid_rotary(values, offset):
    row_count = values.shape[0]
    head_width = values.shape[-1]
    quarter = head_width // 4
    half_width = head_width // 2
    position = offset + jnp.arange(row_count, dtype=jnp.int32)
    grid_row = (position // GRID_W).astype(jnp.float32)
    grid_col = (position % GRID_W).astype(jnp.float32)
    inverse = ROPE_BASE ** (-jnp.arange(quarter, dtype=jnp.float32) / quarter)
    return jnp.concatenate([rotate_half(values[..., :half_width], grid_row[:, None] * inverse[None, :]), rotate_half(values[..., half_width:], grid_col[:, None] * inverse[None, :])], axis=-1)

def slot_table(route_rows, expert_count, capacity):
    token_count, top_count = route_rows.shape
    flat_routes = route_rows.reshape(-1).astype(jnp.int32)
    one_hot = (flat_routes[:, None] == jnp.arange(expert_count, dtype=jnp.int32)[None, :]).astype(jnp.int32)
    ranked = lax.optimization_barrier(jnp.sum((jnp.cumsum(one_hot, axis=0) - 1) * one_hot, axis=1))
    placed = (flat_routes * capacity + ranked).astype(jnp.int32)
    slot_owner = jnp.full((expert_count * capacity,), token_count * top_count, dtype=jnp.int32)
    slot_owner = slot_owner.at[placed].set(jnp.arange(token_count * top_count, dtype=jnp.int32))
    return (slot_owner, placed)

def mixer_half(q_in, k_in, v_in, q_gain, k_gain, w_out, post_gain):
    queries = head_norm(q_in.astype(jnp.float32).reshape(SEQ, HEADS, HEAD), q_gain.astype(jnp.float32))
    queries = grid_rotary(queries, 0).astype(jnp.bfloat16)
    keys = head_norm(k_in.astype(jnp.float32).reshape(SEQ, KV_HEADS, HEAD), k_gain.astype(jnp.float32))
    keys = grid_rotary(keys, 0).astype(jnp.bfloat16)
    repeat = HEADS // KV_HEADS
    key_float = keys.astype(jnp.float32)
    value_float = v_in.astype(jnp.float32).reshape(SEQ, KV_HEADS, HEAD)
    blocked = queries.reshape(SEQ // 128, 128, KV_HEADS, repeat, HEAD)

    def attend(query_block):
        scores = jnp.einsum('qgrd,kgd->grqk', query_block.astype(jnp.float32), key_float) * HEAD ** (-0.5)
        weights = jnp.exp(scores)
        denominator = lax.optimization_barrier(jnp.sum(weights, axis=-1))
        rounded = lax.optimization_barrier(weights.astype(jnp.bfloat16)).astype(jnp.float32)
        summed = jnp.einsum('grqk,kgd->qgrd', rounded, value_float)
        return (summed / jnp.transpose(denominator, (2, 0, 1))[..., None]).astype(jnp.bfloat16)
    head_out = lax.map(attend, blocked).reshape(SEQ, HEADS * HEAD)
    grouped_out = head_out.reshape(SEQ, N_TP, HEADS_DEV * HEAD)
    grouped_w = w_out.reshape(N_TP, HEADS_DEV * HEAD, D)

    def add_group(running, index):
        term = jnp.dot(grouped_out[:, index], grouped_w[index], preferred_element_type=jnp.float32)
        term = lax.optimization_barrier(term.astype(jnp.bfloat16))
        return (running + term.astype(jnp.float32), None)
    mixed, unused = lax.scan(add_group, jnp.zeros((SEQ, D), jnp.float32), jnp.arange(N_TP, dtype=jnp.int32))
    return head_norm(mixed, post_gain.astype(jnp.float32)).astype(jnp.bfloat16)

def experts_half(moe_in, routes, route_logits, pre_gain, w_gate, w_up, w_down):
    normed = head_norm(moe_in.astype(jnp.float32), pre_gain.astype(jnp.float32)).astype(jnp.bfloat16)
    copy_count = TOKM * TOP
    local_copies = TOKM_DEV * TOP
    padded = jnp.concatenate([normed, jnp.zeros((1, D), normed.dtype)], axis=0)
    blocks = routes.reshape(N_EP, TOKM_DEV, TOP)
    owners, unused = jax.vmap(lambda block_routes: slot_table(block_routes, EXPERTS, CAP))(blocks)
    shift_by = (jnp.arange(N_EP, dtype=jnp.int32) * local_copies)[:, None]
    global_owner = jnp.where(owners < local_copies, owners + shift_by, copy_count).astype(jnp.int32)
    per_expert = global_owner.reshape(N_EP, EXPERTS, CAP).transpose(1, 0, 2).reshape(EXPERTS, N_EP * CAP)

    def one_expert(results, inputs):
        owner_ids, gate_w, up_w, down_w = inputs
        gathered = padded[owner_ids // TOP]
        gate_pre = jnp.dot(gathered, gate_w, preferred_element_type=jnp.float32)
        up_pre = jnp.dot(gathered, up_w, preferred_element_type=jnp.float32)
        hidden = (jax.nn.silu(gate_pre) * up_pre).astype(jnp.bfloat16)
        hidden_groups = hidden.reshape(N_EP * CAP, N_TP, FF_DEV)
        down_groups = down_w.reshape(N_TP, FF_DEV, D)

        def add_group(running, index):
            term = jnp.dot(hidden_groups[:, index], down_groups[index], preferred_element_type=jnp.float32)
            term = lax.optimization_barrier(term.astype(jnp.bfloat16))
            return (running + term.astype(jnp.float32), None)
        combined, unused_out = lax.scan(add_group, jnp.zeros((N_EP * CAP, D), jnp.float32), jnp.arange(N_TP, dtype=jnp.int32))
        return (results.at[owner_ids].set(combined.astype(results.dtype)), None)
    results, unused_all = lax.scan(one_expert, jnp.zeros((copy_count + 1, D), jnp.bfloat16), (per_expert, w_gate, w_up, w_down))
    copies = results[:copy_count].reshape(TOKM, TOP, D).astype(jnp.float32)
    route_weight = jax.nn.softmax(route_logits.astype(jnp.float32), axis=-1)
    return lax.optimization_barrier(jnp.sum(route_weight[..., None] * copies, axis=1)).astype(jnp.bfloat16)

def reference(q_in, k_in, v_in, q_gain, k_gain, w_out, post_gain, moe_in, routes, route_logits, pre_gain, w_gate, w_up, w_down):
    attn_out = mixer_half(q_in, k_in, v_in, q_gain, k_gain, w_out, post_gain)
    moe_out = experts_half(moe_in, routes, route_logits, pre_gain, w_gate, w_up, w_down)
    return (attn_out, moe_out)
```

```python
import functools

import jax
import jax.numpy as jnp
from jax import lax
from jax.experimental import pallas as pl
from jax.experimental.pallas import tpu as pltpu
from jax.sharding import Mesh
from jax.sharding import PartitionSpec as P

GRID_W = 128
EPSILON = 1e-06
ROPE_BASE = 10000.0
EP = ("z", "x")
TP = ("y", "c")
ALL = ("z", "x", "y", "c")
NY = 8
ODIM = 80
MESH = pl.DeviceIdType.MESH
BF = jnp.bfloat16
F32 = jnp.float32


def head_norm(values, gain):
    return values * lax.rsqrt(jnp.mean(values * values, axis=-1, keepdims=True) + EPSILON) * gain


def rotate_half(values, angles):
    quarter = angles.shape[-1]
    a = values[..., :quarter]
    b = values[..., quarter:]
    cosine = jnp.cos(angles)
    sine = jnp.sin(angles)
    return jnp.concatenate([a * cosine - b * sine, b * cosine + a * sine], axis=-1)


def grid_rotary(values, offset):
    rows, width = values.shape
    quarter = width // 4
    half = width // 2
    position = offset + jnp.arange(rows, dtype=jnp.int32)
    grid_row = (position // GRID_W).astype(F32)
    grid_col = (position % GRID_W).astype(F32)
    inverse = ROPE_BASE ** (-jnp.arange(quarter, dtype=F32) / quarter)
    return jnp.concatenate(
        [
            rotate_half(values[:, :half], grid_row[:, None] * inverse[None, :]),
            rotate_half(values[:, half:], grid_col[:, None] * inverse[None, :]),
        ],
        axis=-1,
    )


def dot(a, b):
    return jnp.dot(a, b, preferred_element_type=F32)


def dot_t(a, b):
    return lax.dot_general(a, b, (((0,), (0,)), ((), ())), preferred_element_type=F32)


def kernel(
    nz, nx, cap,
    q_ref, kv_ref, og_ref, pf_ref, pb_ref, pg_ref, wg_hbm, wu_hbm, wd_hbm, wo_hbm,
    out_ref, fin_ref,
    kvb, qb, qd, acc, ob, orx, wob, pa, ra,
    zrx, xsb, xb, wg, wu, wd, ga, up, tmp, own, pbuf, prx, psb, rs, ret, rbk, t2, fin,
    lsem, kxs, kxr, rrs, rrr, rls, rlr, qs, qr, ts, tr, wos, wor, as_, ar,
    zs, zr, xs, xr, ys, yr, ds, dr, es, er, ms, mr, vs, vr, us, ur,
):
    z, x, y, c = (lax.axis_index(n) for n in ALL)
    rows = nz * nx * cap
    zb, xbk = nx * cap, nz * cap
    b = lax.rem(y, 2)
    h = y // 2
    m = b * 2 + c
    ysw = y + 1 - 2 * b
    oc = 1 - c
    sgn = 1 - 2 * c

    def yy(k):
        return lax.rem(y + (k + 2 * NY), NY)

    def zz(k):
        return lax.rem(z + (k + nz), nz)

    def xx(k):
        return lax.rem(x + (k + nx), nx)

    sent = []

    def rc(src, dst, ss, rr, dz=None, dx=None, dy=None, dc=None):
        dev = (z if dz is None else dz, x if dx is None else dx, y if dy is None else dy, c if dc is None else dc)
        return pltpu.make_async_remote_copy(src, dst, ss, rr, device_id=dev, device_id_type=MESH)

    def send(*args, **kw):
        copy = rc(*args, **kw)
        copy.start()
        sent.append(copy)

    def local(src, dst, i):
        copy = pltpu.make_async_copy(src, dst, lsem.at[i])
        copy.start()
        return copy

    lwo = local(wo_hbm, wob.at[m], 0)
    lwg = local(wg_hbm, wg, 1)
    lwu = local(wu_hbm, wu, 2)
    lwd = [local(wd_hbm.at[:, k * 256 : (k + 1) * 256], wd.at[k], 3 + k) for k in range(NY)]

    bar = pltpu.get_barrier_semaphore()
    peers = [(zz(k), x, y, c) for k in range(1, nz)]
    peers += [(z, xx(k), y, c) for k in range(1, nx)]
    peers += [(z, x, yy(k), c) for k in (1, -1, 2, -2, 4)]
    peers += [(z, x, y, oc), (z, x, ysw, oc)]
    for peer in peers:
        pl.semaphore_signal(bar, inc=1, device_id=peer, device_id_type=MESH)
    kvb[z, x] = kv_ref[...]
    qb[m] = q_ref[...]
    zrow = pl.multiple_of(z * zb, 16)
    zrx[pl.ds(zrow, zb), :] = og_ref[pl.ds(zrow, zb), :]
    pl.semaphore_wait(bar, len(peers))

    for k in range(1, nx):
        send(kv_ref, kvb.at[z, x], kxs.at[k], kxr.at[k], dx=xx(k))
    for k in range(1, nz):
        to = pl.multiple_of(zz(k) * zb, 16)
        send(og_ref.at[pl.ds(to, zb)], zrx.at[pl.ds(zrow, zb)], zs.at[k], zr.at[k], dz=zz(k))
    send(q_ref, qb.at[m], qs.at[0], qr.at[0], dc=oc)
    send(q_ref, qb.at[m], qs.at[1], qr.at[1], dy=ysw)
    send(q_ref, qb.at[m], qs.at[2], qr.at[2], dy=ysw, dc=oc)

    for j in range(8):
        qd[j] = jnp.zeros((128, 512), BF)
        acc[j] = jnp.zeros((ODIM, 256), F32)

    for k in range(1, nx):
        rc(kv_ref, kvb.at[z, xx(-k)], kxs.at[k], kxr.at[k]).wait_recv()

    def ring(step):
        if step < nz // 2:
            g = kvb.at[zz(-step)]
            send(g, g, rrs.at[step], rrr.at[step], dz=zz(1))
        if step < (nz - 1) // 2:
            g = kvb.at[zz(step)]
            send(g, g, rls.at[step], rlr.at[step], dz=zz(-1))

    def ring_wait(step):
        got = []
        if step < nz // 2:
            g = kvb.at[zz(-step - 1)]
            rc(g, g, rrs.at[step], rrr.at[step]).wait_recv()
            got.append(zz(-step - 1))
        if step < (nz - 1) // 2:
            g = kvb.at[zz(step + 1)]
            rc(g, g, rls.at[step], rlr.at[step]).wait_recv()
            got.append(zz(step + 1))
        return got

    ring(0)

    for k in range(1, nz):
        frm = pl.multiple_of(zz(-k) * zb, 16)
        rc(og_ref.at[pl.ds(0, zb)], zrx.at[pl.ds(frm, zb)], zs.at[k], zr.at[k]).wait_recv()
    xsb[...] = dot(pf_ref[...], zrx[...]).astype(BF)
    cl = pl.multiple_of(c * 128, 128)
    ocl = pl.multiple_of(oc * 128, 128)
    xrow = pl.multiple_of(x * xbk, 16)
    slots = (yy(0), yy(4))
    for i in range(2):
        xb[slots[i], pl.ds(xrow, xbk), pl.ds(cl, 128)] = xsb[pl.ds(xrow, xbk), i * 128 : (i + 1) * 128]
    for k in range(1, nx):
        to = pl.multiple_of(xx(k) * xbk, 16)
        for i in range(2):
            send(
                xsb.at[pl.ds(to, xbk), pl.ds(i * 128, 128)],
                xb.at[slots[i], pl.ds(xrow, xbk), pl.ds(cl, 128)],
                xs.at[i, k], xr.at[i, k], dx=xx(k),
            )

    rc(q_ref, qb.at[b * 2 + oc], qs.at[0], qr.at[0]).wait_recv()
    rc(q_ref, qb.at[(1 - b) * 2 + c], qs.at[1], qr.at[1]).wait_recv()
    rc(q_ref, qb.at[(1 - b) * 2 + oc], qs.at[2], qr.at[2]).wait_recv()
    for mt in range(4):
        for rp in range(2):
            pair = [qb[2 * rp + i, :, mt * 128 : (mt + 1) * 128] for i in range(2)]
            pair = jnp.concatenate(pair, axis=1)
            qd[mt * 2 + rp, 0:64, 0:256] = pair
            qd[mt * 2 + rp, 64:128, 256:512] = pair

    def attend(zi):
        keys = kvb[zi, :, 0:64, :].reshape(nx * 64, 128)
        vals = [kvb[zi, i, 64:128, :] for i in range(nx)]
        vals = jnp.concatenate(vals, axis=1)
        vals = jnp.concatenate([vals, jnp.ones((ODIM - 64, nx * 128), BF)], axis=0)

        def tile(j, carry):
            p = jnp.exp(dot(keys, qd[j])).astype(BF)
            parts = []
            for i in range(nx):
                parts.append(p[i * 64 : (i + 1) * 64, 0:256])
                parts.append(p[i * 64 : (i + 1) * 64, 256:512])
            acc[j] += dot(vals, jnp.concatenate(parts, axis=0))
            return carry

        lax.fori_loop(0, 8, tile, 0)

    attend(z)

    for k in range(1, nx):
        frm = pl.multiple_of(xx(-k) * xbk, 16)
        for i in range(2):
            rc(
                xsb.at[pl.ds(0, xbk), pl.ds(i * 128, 128)],
                xb.at[slots[i], pl.ds(frm, xbk), pl.ds(cl, 128)],
                xs.at[i, k], xr.at[i, k],
            ).wait_recv()

    def half(slot, which):
        return xb.at[slot, :, pl.ds(which, 128)]

    plan = ((1, 0), (1, 4), (-1, 0), (-1, 4), (2, 0), (-2, 0))
    for i, (k, r) in enumerate(plan):
        g = half(yy(r), cl)
        send(g, g, ys.at[i], yr.at[i], dy=yy(k))

    def swap(r):
        g = half(yy(r), cl)
        send(g, g, ds.at[r], dr.at[r], dc=oc)

    swap(0)
    swap(4)
    lwo.wait()
    send(wob.at[m], wob.at[m], wos.at[0], wor.at[0], dc=oc)
    send(wob.at[m], wob.at[m], wos.at[1], wor.at[1], dy=ysw)

    def arrive(i):
        k, r = plan[i]
        g = half(yy(r - k), cl)
        rc(g, g, ys.at[i], yr.at[i]).wait_recv()
        swap((r - k + NY) % NY)

    steps = max(nz // 2, (nz - 1) // 2)
    for step in range(steps):
        got = ring_wait(step)
        ring(step + 1)
        if step == steps - 2:
            for i in range(4):
                arrive(i)
        for zi in got:
            attend(zi)
    if steps < 2:
        for i in range(4):
            arrive(i)
    for i in range(4, 6):
        arrive(i)

    for j in range(8):
        a = acc[j]
        den = a[64:ODIM]
        hi = den.astype(BF)
        lo = (den - hi.astype(F32)).astype(BF)
        first = lax.broadcasted_iota(jnp.int32, (ODIM - 64, 256), 0) == 0
        ob[j, 0:64] = a[0:64].astype(BF)
        ob[j, 64:ODIM] = jnp.where(first, hi.astype(F32), lo.astype(F32)).astype(BF)
    other = wob.at[(1 - b) * 2 + c]
    rc(other, other, wos.at[1], wor.at[1]).wait_recv()
    send(other, other, wos.at[2], wor.at[2], dc=oc)
    members = ((0, y, oc, b * 2 + oc), (1, ysw, c, (1 - b) * 2 + c), (2, ysw, oc, (1 - b) * 2 + oc))
    for i, dy, dc, mm in members:
        send(ob.at[pl.ds(2 * mm, 2)], orx.at[i], ts.at[i], tr.at[i], dy=dy, dc=dc)

    lwg.wait()
    lwu.wait()
    for i, r in enumerate((0, 4, 1, 5, 7, 3, 2, 6)):
        s = yy(r)
        g = half(s, ocl)
        rc(g, g, ds.at[r], dr.at[r]).wait_recv()
        w0 = pl.multiple_of(s * 256, 256)
        gd = dot(xb[s], wg[pl.ds(w0, 256), :])
        ud = dot(xb[s], wu[pl.ds(w0, 256), :])
        if i == 0:
            ga[...] = gd
            up[...] = ud
        else:
            ga[...] += gd
            up[...] += ud
    gate = ga[...]
    hid = (gate / (1.0 + jnp.exp(-gate)) * up[...]).astype(BF)
    for copy in lwd:
        copy.wait()
    order = (4, 3, 5, 1, 7, 2, 6, 0)
    for r in order:
        tmp[r % 2] = dot(hid, wd[yy(r)])
        own[r] = tmp[r % 2, :, pl.ds(cl, 128)]
        pbuf[r] = tmp[r % 2, :, pl.ds(ocl, 128)].astype(BF)
        send(pbuf.at[r], prx.at[r], es.at[r], er.at[r], dc=oc)

    def paired(r):
        rc(pbuf.at[r], prx.at[r], es.at[r], er.at[r]).wait_recv()
        return own[r] + prx[r].astype(F32)

    for r, i, dest in ((4, 0, yy(0 - 2 * sgn)), (3, 1, yy(1)), (5, 2, yy(-1)), (1, 3, yy(1)), (7, 4, yy(-1))):
        psb[r] = paired(r).astype(BF)
        send(psb.at[r], rs.at[i], ms.at[i], mr.at[i], dy=dest)

    def got_rs(i):
        rc(psb.at[0], rs.at[i], ms.at[i], mr.at[i]).wait_recv()
        return rs[i].astype(F32)

    for i, dy, dc, mm in members:
        rc(ob.at[pl.ds(0, 2)], orx.at[i], ts.at[i], tr.at[i]).wait_recv()
    heads = []
    for rp in range(2):
        t = ob[2 * m + rp].astype(F32)
        for i in range(3):
            t += orx[i, rp].astype(F32)
        o = (t[0:64] / (t[64:65] + t[65:66])).astype(BF)
        heads += [o[:, 0:128], o[:, 128:256]]
    hot = jnp.concatenate(heads, axis=0)
    partner = wob.at[b * 2 + oc]
    rc(partner, partner, wos.at[0], wor.at[0]).wait_recv()
    far = wob.at[(1 - b) * 2 + oc]
    rc(far, far, wos.at[2], wor.at[2]).wait_recv()
    for n in range(4):
        part = dot_t(hot, wob[:, :, n * 512 : (n + 1) * 512].reshape(256, 512))
        pa[:, :, n * 512 : (n + 1) * 512] = part.astype(BF).reshape(4, 32, 512)

    far_sum = got_rs(0)
    right = c.astype(F32)
    psb[2] = (paired(2) + got_rs(1) + far_sum * right).astype(BF)
    send(psb.at[2], rs.at[5], ms.at[5], mr.at[5], dy=yy(2))
    psb[6] = (paired(6) + got_rs(2) + far_sum * (1.0 - right)).astype(BF)
    send(psb.at[6], rs.at[6], ms.at[6], mr.at[6], dy=yy(-2))

    for k in range(1, 4):
        send(pa.at[lax.rem(h + k, 4)], ra.at[k - 1], as_.at[k - 1], ar.at[k - 1], dy=yy(2 * k))

    ret[...] = (paired(0) + got_rs(3) + got_rs(4) + got_rs(5) + got_rs(6)).astype(BF)
    rbk[pl.ds(xrow, xbk), :] = ret[pl.ds(xrow, xbk), :]
    for k in range(1, nx):
        to = pl.multiple_of(xx(k) * xbk, 16)
        send(ret.at[pl.ds(to, xbk)], rbk.at[pl.ds(xrow, xbk)], vs.at[k], vr.at[k], dx=xx(k))
    for k in range(1, nx):
        frm = pl.multiple_of(xx(-k) * xbk, 16)
        rc(ret.at[pl.ds(0, xbk)], rbk.at[pl.ds(frm, xbk)], vs.at[k], vr.at[k]).wait_recv()
    t2[...] = dot(pb_ref[...], rbk[...]).astype(BF)
    fin[pl.ds(zrow, zb), :] = t2[pl.ds(zrow, zb), :]
    for k in range(1, nz):
        to = pl.multiple_of(zz(k) * zb, 16)
        send(t2.at[pl.ds(to, zb)], fin.at[pl.ds(zrow, zb)], us.at[k], ur.at[k], dz=zz(k))

    mixed = pa[h].astype(F32)
    for k in range(1, 4):
        rc(pa.at[0], ra.at[k - 1], as_.at[k - 1], ar.at[k - 1]).wait_recv()
        mixed += ra[k - 1].astype(F32)
    scale = lax.rsqrt(jnp.mean(mixed * mixed, axis=1, keepdims=True) + EPSILON)
    out_ref[...] = (mixed * scale * pg_ref[...]).astype(BF)

    for k in range(1, nz):
        frm = pl.multiple_of(zz(-k) * zb, 16)
        rc(t2.at[pl.ds(0, zb)], fin.at[pl.ds(frm, zb)], us.at[k], ur.at[k]).wait_recv()
    fin_ref[...] = fin[...]
    for copy in sent:
        copy.wait_send()


def call(nz, nx, cap, *args):
    rows = nz * nx * cap
    vm = pl.BlockSpec(memory_space=pltpu.VMEM)
    hbm = pl.BlockSpec(memory_space=pl.ANY)
    dma = lambda *n: pltpu.SemaphoreType.DMA(n)
    big = lambda *s: pltpu.VMEM(s, BF)
    wide = lambda *s: pltpu.VMEM(s, F32)
    scratch = [
        big(nz, nx, 128, 128), big(4, 64, 512), big(8, 128, 512), wide(8, ODIM, 256), big(8, ODIM, 256),
        big(3, 2, ODIM, 256), big(4, 64, 2048), big(4, 32, 2048), big(3, 32, 2048),
        big(rows, 256), big(rows, 256), big(NY, rows, 256), big(2048, 256), big(2048, 256), big(NY, 256, 256),
        wide(rows, 256), wide(rows, 256), wide(2, rows, 256), wide(NY, rows, 128), big(NY, rows, 128),
        big(NY, rows, 128), big(NY, rows, 128), big(7, rows, 128), big(rows, 128), big(rows, 128),
        big(rows, 128), big(rows, 128),
        dma(11), dma(nx), dma(nx), dma(nz), dma(nz), dma(nz), dma(nz), dma(3), dma(3), dma(3), dma(3), dma(3), dma(3),
        dma(3), dma(3),
        dma(nz), dma(nz), dma(2, nx), dma(2, nx), dma(6), dma(6), dma(8), dma(8), dma(8), dma(8), dma(7), dma(7),
        dma(nx), dma(nx), dma(nz), dma(nz),
    ]
    return pl.pallas_call(
        functools.partial(kernel, nz, nx, cap),
        out_shape=(jax.ShapeDtypeStruct((32, 2048), BF), jax.ShapeDtypeStruct((rows, 128), BF)),
        in_specs=[vm] * 6 + [hbm] * 4,
        out_specs=(vm, vm),
        scratch_shapes=scratch,
        compiler_params=pltpu.CompilerParams(
            collective_id=0, has_side_effects=True, vmem_limit_bytes=48 * 1024 * 1024
        ),
        name="layer",
    )(*args)


def per_device(
    q_in, k_in, v_in, q_gain, k_gain, w_out, post_gain, moe_in, routes, route_logits, pre_gain, w_gate, w_up, w_down
):
    nz, nx = lax.axis_size("z"), lax.axis_size("x")
    y, c = lax.axis_index("y"), lax.axis_index("c")
    ep = lax.axis_index(EP)
    count, top = routes.shape
    experts = nz * nx
    cap = max(2, 3 * top * count // (2 * experts))
    rows = experts * cap
    offset = ep * 512
    h = y // 2
    m = lax.rem(y, 2) * 2 + c

    q = grid_rotary(head_norm(q_in.astype(F32), q_gain), offset).astype(BF) * BF(0.125)
    q = jnp.transpose(q.reshape(4, 4, 32, 64), (3, 1, 0, 2)).reshape(64, 512)
    k = lax.dynamic_slice(k_in, (m * 128, h * 64), (128, 64)).astype(F32)
    k = grid_rotary(head_norm(k, k_gain), offset + m * 128).astype(BF)
    v = lax.dynamic_slice(v_in, (m * 128, h * 64), (128, 64))
    kv = jnp.concatenate([jnp.concatenate([k[:64], k[64:]], axis=1), v.T], axis=0)

    x32 = moe_in.astype(F32)
    scale = lax.rsqrt(jnp.mean(x32 * x32, axis=-1, keepdims=True) + EPSILON)
    cols = [(lax.rem(y + 4 * i, NY) * 2 + c) * 128 for i in range(2)]
    xs = [lax.dynamic_slice(moe_in, (0, col), (count, 128)).astype(F32) for col in cols]
    gs = [lax.dynamic_slice(pre_gain, (col,), (128,)) for col in cols]
    xn = jnp.concatenate([(v_ * scale * g_).astype(BF) for v_, g_ in zip(xs, gs)], axis=1)
    rt = routes.T
    eid = jnp.arange(experts, dtype=jnp.int32)[:, None]
    hot = [(eid == rt[i][None, :]) for i in range(top)]
    both = (hot[0] | hot[1]).astype(BF)
    tri = (jnp.arange(count)[:, None] < jnp.arange(count)[None, :]).astype(BF)
    rank = dot(both, tri).astype(jnp.int32)
    place = [jnp.sum(jnp.where(hh, rank + cap * eid, 0), axis=0) for hh in hot]
    slot = jnp.arange(rows, dtype=jnp.int32)[:, None]
    sel = [(slot == pp[None, :]) for pp in place]
    og = dot((sel[0] | sel[1]).astype(BF), xn).astype(BF)

    i = jnp.arange(rows, dtype=jnp.int32)
    src = (i % (nz * cap)) // cap * (nx * cap) + i // (nz * cap) * cap + i % cap
    pf = (src[:, None] == i[None, :]).astype(BF)
    pb = (src[None, :] == i[:, None]).astype(BF)

    attn, fin = call(
        nz, nx, cap, q, kv, og, pf, pb, post_gain[None, :], w_gate[0], w_up[0], w_down[0], w_out
    )
    weight = jax.nn.softmax(route_logits, axis=-1)
    moe = sum(weight[:, j : j + 1] * dot_t(sel[j].astype(BF), fin) for j in range(top))
    return attn, moe.astype(BF)


def solution(mesh):
    ny = mesh.shape["tp"] // 2
    nz = 8 if mesh.shape["ep"] % 8 == 0 else 2
    finer = Mesh(mesh.devices.reshape(nz, mesh.shape["ep"] // nz, ny, 2), ALL)
    in_specs = (
        P(EP, TP), P(EP, None), P(EP, None), P(), P(), P(TP, None), P(), P(EP, None), P(EP, None), P(EP, None), P(),
        P(EP, None, TP), P(EP, None, TP), P(EP, TP, None),
    )
    return jax.shard_map(
        per_device, mesh=finer, in_specs=in_specs, out_specs=(P(ALL, None), P(EP, TP)), check_vma=False
    )
```

```python
import functools

import jax
import jax.numpy as jnp
import numpy as np
from jax import lax
from jax.experimental import pallas as pl
from jax.experimental.pallas import tpu as pltpu
from jax.sharding import Mesh
from jax.sharding import PartitionSpec as P

GRID_W = 128
EPSILON = 1e-06
ROPE_BASE = 10000.0
EP = ("z", "x")
TP = ("y", "c")
ALL = ("z", "x", "y", "c")
NY = 8
ODIM = 80
MESH = pl.DeviceIdType.MESH
BF = jnp.bfloat16
F32 = jnp.float32


def angle_table():
    lane = np.arange(128)
    inverse = np.float32(ROPE_BASE) ** (-np.arange(16, dtype=np.float32) / np.float32(16))
    angle = (np.arange(GRID_W, dtype=np.float32)[:, None] * inverse[None, lane % 16]).astype(np.float64)
    sign = np.where(lane % 32 < 16, -1.0, 1.0)[None, :]
    return np.where(lane[None, :] < 64, np.cos(angle), sign * np.sin(angle)).astype(np.float32)


def dot(a, b):
    return jnp.dot(a, b, preferred_element_type=F32)


def dot_t(a, b):
    return lax.dot_general(a, b, (((0,), (0,)), ((), ())), preferred_element_type=F32)


def dot_nt(a, b):
    return lax.dot_general(a, b, (((1,), (1,)), ((), ())), preferred_element_type=F32)


def iota(shape, dim):
    return lax.broadcasted_iota(jnp.int32, shape, dim)


def kernel(
    nz, nx, cap,
    tab_ref, qg_ref, kg_ref, rt_ref, lg_ref, src_ref, pre_hbm, post_hbm, q_hbm, k_hbm, v_hbm, x_hbm, wg_hbm, wu_hbm, wd_hbm, wo_hbm,
    out_ref, moe_ref,
    qv, kv, vv, xv, prev, pg_ref, q_ref, kv_ref, og_ref, pb_ref,
    kvb, qb, qd, acc, ob, orx, wob, pa, ra,
    zrx, xsb, xb, wg, wu, wd, ga, up, tmp, own, pbuf, prx, psb, rs, ret, rbk, t2, fin,
    lsem, kxs, kxr, rrs, rrr, rls, rlr, qs, qr, ts, tr, wos, wor, as_, ar,
    zs, zr, xs, xr, ys, yr, ds, dr, es, er, ms, mr, vs, vr, us, ur,
):
    z, x, y, c = (lax.axis_index(n) for n in ALL)
    rows = nz * nx * cap
    zb, xbk = nx * cap, nz * cap
    b = lax.rem(y, 2)
    h = y // 2
    m = b * 2 + c
    ysw = y + 1 - 2 * b
    oc = 1 - c
    sgn = 1 - 2 * c

    def yy(k):
        return lax.rem(y + (k + 2 * NY), NY)

    def zz(k):
        return lax.rem(z + (k + nz), nz)

    def xx(k):
        return lax.rem(x + (k + nx), nx)

    sent = []

    def rc(src, dst, ss, rr, dz=None, dx=None, dy=None, dc=None):
        dev = (z if dz is None else dz, x if dx is None else dx, y if dy is None else dy, c if dc is None else dc)
        return pltpu.make_async_remote_copy(src, dst, ss, rr, device_id=dev, device_id_type=MESH)

    def send(*args, **kw):
        copy = rc(*args, **kw)
        copy.start()
        sent.append(copy)

    def local(src, dst, i):
        copy = pltpu.make_async_copy(src, dst, lsem.at[i])
        copy.start()
        return copy

    ep = z * nx + x
    hl = pl.multiple_of((h // 2) * 128, 128)
    mrow = pl.multiple_of(m * 128, 128)
    lk = local(k_hbm.at[pl.ds(mrow, 128), pl.ds(hl, 128)], kv, 11)
    lv = local(v_hbm.at[pl.ds(mrow, 128), pl.ds(hl, 128)], vv, 12)
    lx = local(x_hbm, xv, 13)
    lq = local(q_hbm, qv, 14)
    lpre = local(pre_hbm, prev, 15)
    lpost = local(post_hbm, pg_ref, 16)
    lwo = local(wo_hbm, wob.at[m], 0)
    lwg = local(wg_hbm, wg, 1)
    lwu = local(wu_hbm, wu, 2)
    lwd = [local(wd_hbm.at[:, k * 256 : (k + 1) * 256], wd.at[k], 3 + k) for k in range(NY)]

    bar = pltpu.get_barrier_semaphore()
    peers = [(zz(k), x, y, c) for k in range(1, nz)]
    peers += [(z, xx(k), y, c) for k in range(1, nx)]
    peers += [(z, x, yy(k), c) for k in (1, -1, 2, -2, 4)]
    peers += [(z, x, y, oc), (z, x, ysw, oc)]
    for peer in peers:
        pl.semaphore_signal(bar, inc=1, device_id=peer, device_id_type=MESH)

    def mixer(j, l):
        i = j - 64
        return ((l < 64) & (i == l)) | ((l >= 64) & (i == ((l - 64) ^ 16)))

    wide_mix = mixer(iota((192, 128), 0), iota((192, 128), 1)).astype(F32).astype(BF)
    sub = lax.rem(h, 2)
    hmix = mixer(iota((128, 128), 0) + (1 - sub) * 64, iota((128, 128), 1)).astype(F32).astype(BF)
    qmix = wide_mix[64:128]
    lane = iota((128, 128), 1)
    row_lane = (lane & 63) < 32
    col_table = tab_ref[...]

    def gains(ref):
        return jnp.dot(
            jnp.broadcast_to(ref[...], (8, 64)), qmix.astype(F32), precision=lax.Precision.HIGHEST,
            preferred_element_type=F32,
        )[0:1]

    def turned(values, gain, r):
        table = jnp.where(row_lane, tab_ref[pl.ds(r, 1), :], col_table) * gain
        scale = lax.rsqrt(jnp.mean(values * values, axis=1, keepdims=True) + EPSILON)
        out = values * scale * table
        return out + pltpu.roll(out, 64, 1)

    kgain = gains(kg_ref)
    lk.wait()
    k128 = turned(dot(kv[...], hmix), kgain, ep * 4 + m)
    kv_ref[0:64] = jnp.where(lane[0:64] < 64, k128[0:64], k128[64:128]).astype(BF)
    lv.wait()
    pick = (iota((64, 128), 1) == iota((64, 128), 0) + 64 * sub).astype(F32).astype(BF)
    kv_ref[64:128] = dot_nt(pick, vv[...]).astype(BF)
    kvb[z, x] = kv_ref[...]

    count = xv.shape[0]
    experts = nz * nx
    lx.wait()
    x32 = xv[...].astype(F32)
    xscale = lax.rsqrt(jnp.mean(x32 * x32, axis=1, keepdims=True) + EPSILON)
    lpre.wait()
    normed = []
    for i in range(2):
        col = pl.multiple_of((yy(4 * i) * 2 + c) * 128, 128)
        normed.append((xv[:, pl.ds(col, 128)].astype(F32) * xscale * prev[:, pl.ds(col, 128)]).astype(BF))
    normed = jnp.concatenate(normed, axis=1)
    eid = iota((count, 128), 1)
    eye = (iota((count, count), 1) == iota((count, count), 0)).astype(F32)
    named = dot_nt(eye.astype(BF), rt_ref[...].astype(F32).astype(BF)).astype(jnp.int32)
    hot = [eid == named[:, i : i + 1] for i in range(2)]
    lower = (iota((count, count), 1) < iota((count, count), 0)).astype(F32).astype(BF)
    rank = dot(lower, (hot[0] | hot[1]).astype(F32).astype(BF)) + (cap * eid).astype(F32)
    place = [jnp.sum(jnp.where(hh, rank, 0.0), axis=1, keepdims=True).astype(jnp.int32) for hh in hot]
    slot = iota((count, rows), 1)
    pick = [slot == pp for pp in place]
    og_ref[...] = dot_t((pick[0] | pick[1]).astype(F32).astype(BF), normed).astype(BF)
    pb_ref[...] = (iota((rows, rows), 0) == src_ref[...]).astype(F32).astype(BF)

    lq.wait()
    q128 = dot_t(qv[...], qmix)
    qgain = gains(qg_ref)
    turned_q = [turned(q128[i * 128 : (i + 1) * 128], qgain, ep * 4 + i).astype(BF) for i in range(4)]
    ordered = [turned_q[i][k * 32 : (k + 1) * 32] for k in range(4) for i in range(4)]
    ordered = jnp.concatenate(ordered, axis=0) * BF(0.125)
    pick_q = (iota((64, 128), 1) == iota((64, 128), 0)).astype(F32).astype(BF)
    q_ref[...] = dot_nt(pick_q, ordered).astype(BF)
    qb[m] = q_ref[...]
    zrow = pl.multiple_of(z * zb, 16)
    zrx[pl.ds(zrow, zb), :] = og_ref[pl.ds(zrow, zb), :]
    pl.semaphore_wait(bar, len(peers))

    for k in range(1, nx):
        send(kv_ref, kvb.at[z, x], kxs.at[k], kxr.at[k], dx=xx(k))
    for k in range(1, nz):
        to = pl.multiple_of(zz(k) * zb, 16)
        send(og_ref.at[pl.ds(to, zb)], zrx.at[pl.ds(zrow, zb)], zs.at[k], zr.at[k], dz=zz(k))
    send(q_ref, qb.at[m], qs.at[0], qr.at[0], dc=oc)
    send(q_ref, qb.at[m], qs.at[1], qr.at[1], dy=ysw)
    send(q_ref, qb.at[m], qs.at[2], qr.at[2], dy=ysw, dc=oc)

    for j in range(8):
        qd[j] = jnp.zeros((128, 512), BF)
        acc[j] = jnp.zeros((ODIM, 256), F32)

    for k in range(1, nx):
        rc(kv_ref, kvb.at[z, xx(-k)], kxs.at[k], kxr.at[k]).wait_recv()

    def ring(step):
        if step < nz // 2:
            g = kvb.at[zz(-step)]
            send(g, g, rrs.at[step], rrr.at[step], dz=zz(1))
        if step < (nz - 1) // 2:
            g = kvb.at[zz(step)]
            send(g, g, rls.at[step], rlr.at[step], dz=zz(-1))

    def ring_wait(step):
        got = []
        if step < nz // 2:
            g = kvb.at[zz(-step - 1)]
            rc(g, g, rrs.at[step], rrr.at[step]).wait_recv()
            got.append(zz(-step - 1))
        if step < (nz - 1) // 2:
            g = kvb.at[zz(step + 1)]
            rc(g, g, rls.at[step], rlr.at[step]).wait_recv()
            got.append(zz(step + 1))
        return got

    ring(0)

    for k in range(1, nz):
        frm = pl.multiple_of(zz(-k) * zb, 16)
        rc(og_ref.at[pl.ds(0, zb)], zrx.at[pl.ds(frm, zb)], zs.at[k], zr.at[k]).wait_recv()
    xsb[...] = dot_t(pb_ref[...], zrx[...]).astype(BF)
    cl = pl.multiple_of(c * 128, 128)
    ocl = pl.multiple_of(oc * 128, 128)
    xrow = pl.multiple_of(x * xbk, 16)
    slots = (yy(0), yy(4))
    for i in range(2):
        xb[slots[i], pl.ds(xrow, xbk), pl.ds(cl, 128)] = xsb[pl.ds(xrow, xbk), i * 128 : (i + 1) * 128]
    for k in range(1, nx):
        to = pl.multiple_of(xx(k) * xbk, 16)
        for i in range(2):
            send(
                xsb.at[pl.ds(to, xbk), pl.ds(i * 128, 128)],
                xb.at[slots[i], pl.ds(xrow, xbk), pl.ds(cl, 128)],
                xs.at[i, k], xr.at[i, k], dx=xx(k),
            )

    rc(q_ref, qb.at[b * 2 + oc], qs.at[0], qr.at[0]).wait_recv()
    rc(q_ref, qb.at[(1 - b) * 2 + c], qs.at[1], qr.at[1]).wait_recv()
    rc(q_ref, qb.at[(1 - b) * 2 + oc], qs.at[2], qr.at[2]).wait_recv()
    for mt in range(4):
        for rp in range(2):
            pair = [qb[2 * rp + i, :, mt * 128 : (mt + 1) * 128] for i in range(2)]
            pair = jnp.concatenate(pair, axis=1)
            qd[mt * 2 + rp, 0:64, 0:256] = pair
            qd[mt * 2 + rp, 64:128, 256:512] = pair

    def attend(zi):
        keys = kvb[zi, :, 0:64, :].reshape(nx * 64, 128)
        vals = [kvb[zi, i, 64:128, :] for i in range(nx)]
        vals = jnp.concatenate(vals, axis=1)
        vals = jnp.concatenate([vals, jnp.ones((ODIM - 64, nx * 128), BF)], axis=0)

        def tile(j, carry):
            p = jnp.exp(dot(keys, qd[j])).astype(BF)
            parts = []
            for i in range(nx):
                parts.append(p[i * 64 : (i + 1) * 64, 0:256])
                parts.append(p[i * 64 : (i + 1) * 64, 256:512])
            acc[j] += dot(vals, jnp.concatenate(parts, axis=0))
            return carry

        lax.fori_loop(0, 8, tile, 0)

    attend(z)

    for k in range(1, nx):
        frm = pl.multiple_of(xx(-k) * xbk, 16)
        for i in range(2):
            rc(
                xsb.at[pl.ds(0, xbk), pl.ds(i * 128, 128)],
                xb.at[slots[i], pl.ds(frm, xbk), pl.ds(cl, 128)],
                xs.at[i, k], xr.at[i, k],
            ).wait_recv()

    def half(slot, which):
        return xb.at[slot, :, pl.ds(which, 128)]

    plan = ((1, 0), (1, 4), (-1, 0), (-1, 4), (2, 0), (-2, 0))
    for i, (k, r) in enumerate(plan):
        g = half(yy(r), cl)
        send(g, g, ys.at[i], yr.at[i], dy=yy(k))

    def swap(r):
        g = half(yy(r), cl)
        send(g, g, ds.at[r], dr.at[r], dc=oc)

    swap(0)
    swap(4)
    lwo.wait()
    send(wob.at[m], wob.at[m], wos.at[0], wor.at[0], dc=oc)
    send(wob.at[m], wob.at[m], wos.at[1], wor.at[1], dy=ysw)

    def arrive(i):
        k, r = plan[i]
        g = half(yy(r - k), cl)
        rc(g, g, ys.at[i], yr.at[i]).wait_recv()
        swap((r - k + NY) % NY)

    steps = max(nz // 2, (nz - 1) // 2)
    for step in range(steps):
        got = ring_wait(step)
        ring(step + 1)
        if step == steps - 2:
            for i in range(4):
                arrive(i)
        for zi in got:
            attend(zi)
    if steps < 2:
        for i in range(4):
            arrive(i)
    for i in range(4, 6):
        arrive(i)

    for j in range(8):
        a = acc[j]
        den = a[64:ODIM]
        hi = den.astype(BF)
        lo = (den - hi.astype(F32)).astype(BF)
        first = lax.broadcasted_iota(jnp.int32, (ODIM - 64, 256), 0) == 0
        ob[j, 0:64] = a[0:64].astype(BF)
        ob[j, 64:ODIM] = jnp.where(first, hi.astype(F32), lo.astype(F32)).astype(BF)
    other = wob.at[(1 - b) * 2 + c]
    rc(other, other, wos.at[1], wor.at[1]).wait_recv()
    send(other, other, wos.at[2], wor.at[2], dc=oc)
    members = ((0, y, oc, b * 2 + oc), (1, ysw, c, (1 - b) * 2 + c), (2, ysw, oc, (1 - b) * 2 + oc))
    for i, dy, dc, mm in members:
        send(ob.at[pl.ds(2 * mm, 2)], orx.at[i], ts.at[i], tr.at[i], dy=dy, dc=dc)

    lwg.wait()
    lwu.wait()
    for i, r in enumerate((0, 4, 1, 5, 7, 3, 2, 6)):
        s = yy(r)
        g = half(s, ocl)
        rc(g, g, ds.at[r], dr.at[r]).wait_recv()
        w0 = pl.multiple_of(s * 256, 256)
        gd = dot(xb[s], wg[pl.ds(w0, 256), :])
        ud = dot(xb[s], wu[pl.ds(w0, 256), :])
        if i == 0:
            ga[...] = gd
            up[...] = ud
        else:
            ga[...] += gd
            up[...] += ud
    gate = ga[...]
    hid = (gate / (1.0 + jnp.exp(-gate)) * up[...]).astype(BF)
    for copy in lwd:
        copy.wait()
    order = (4, 3, 5, 1, 7, 2, 6, 0)
    for r in order:
        tmp[r % 2] = dot(hid, wd[yy(r)])
        own[r] = tmp[r % 2, :, pl.ds(cl, 128)]
        pbuf[r] = tmp[r % 2, :, pl.ds(ocl, 128)].astype(BF)
        send(pbuf.at[r], prx.at[r], es.at[r], er.at[r], dc=oc)

    def paired(r):
        rc(pbuf.at[r], prx.at[r], es.at[r], er.at[r]).wait_recv()
        return own[r] + prx[r].astype(F32)

    for r, i, dest in ((4, 0, yy(0 - 2 * sgn)), (3, 1, yy(1)), (5, 2, yy(-1)), (1, 3, yy(1)), (7, 4, yy(-1))):
        psb[r] = paired(r).astype(BF)
        send(psb.at[r], rs.at[i], ms.at[i], mr.at[i], dy=dest)

    def got_rs(i):
        rc(psb.at[0], rs.at[i], ms.at[i], mr.at[i]).wait_recv()
        return rs[i].astype(F32)

    for i, dy, dc, mm in members:
        rc(ob.at[pl.ds(0, 2)], orx.at[i], ts.at[i], tr.at[i]).wait_recv()
    heads = []
    for rp in range(2):
        t = ob[2 * m + rp].astype(F32)
        for i in range(3):
            t += orx[i, rp].astype(F32)
        o = (t[0:64] / (t[64:65] + t[65:66])).astype(BF)
        heads += [o[:, 0:128], o[:, 128:256]]
    hot = jnp.concatenate(heads, axis=0)
    partner = wob.at[b * 2 + oc]
    rc(partner, partner, wos.at[0], wor.at[0]).wait_recv()
    far = wob.at[(1 - b) * 2 + oc]
    rc(far, far, wos.at[2], wor.at[2]).wait_recv()
    for n in range(4):
        part = dot_t(hot, wob[:, :, n * 512 : (n + 1) * 512].reshape(256, 512))
        pa[:, :, n * 512 : (n + 1) * 512] = part.astype(BF).reshape(4, 32, 512)

    far_sum = got_rs(0)
    right = c.astype(F32)
    psb[2] = (paired(2) + got_rs(1) + far_sum * right).astype(BF)
    send(psb.at[2], rs.at[5], ms.at[5], mr.at[5], dy=yy(2))
    psb[6] = (paired(6) + got_rs(2) + far_sum * (1.0 - right)).astype(BF)
    send(psb.at[6], rs.at[6], ms.at[6], mr.at[6], dy=yy(-2))

    for k in range(1, 4):
        send(pa.at[lax.rem(h + k, 4)], ra.at[k - 1], as_.at[k - 1], ar.at[k - 1], dy=yy(2 * k))

    ret[...] = (paired(0) + got_rs(3) + got_rs(4) + got_rs(5) + got_rs(6)).astype(BF)
    rbk[pl.ds(xrow, xbk), :] = ret[pl.ds(xrow, xbk), :]
    for k in range(1, nx):
        to = pl.multiple_of(xx(k) * xbk, 16)
        send(ret.at[pl.ds(to, xbk)], rbk.at[pl.ds(xrow, xbk)], vs.at[k], vr.at[k], dx=xx(k))
    for k in range(1, nx):
        frm = pl.multiple_of(xx(-k) * xbk, 16)
        rc(ret.at[pl.ds(0, xbk)], rbk.at[pl.ds(frm, xbk)], vs.at[k], vr.at[k]).wait_recv()
    t2[...] = dot(pb_ref[...], rbk[...]).astype(BF)
    fin[pl.ds(zrow, zb), :] = t2[pl.ds(zrow, zb), :]
    for k in range(1, nz):
        to = pl.multiple_of(zz(k) * zb, 16)
        send(t2.at[pl.ds(to, zb)], fin.at[pl.ds(zrow, zb)], us.at[k], ur.at[k], dz=zz(k))

    mixed = pa[h].astype(F32)
    for k in range(1, 4):
        rc(pa.at[0], ra.at[k - 1], as_.at[k - 1], ar.at[k - 1]).wait_recv()
        mixed += ra[k - 1].astype(F32)
    scale = lax.rsqrt(jnp.mean(mixed * mixed, axis=1, keepdims=True) + EPSILON)
    lpost.wait()
    out_ref[...] = (mixed * scale * pg_ref[...]).astype(BF)

    logits = lg_ref[...]
    grown = jnp.exp(logits - jnp.max(logits, axis=0, keepdims=True))
    weight = lax.dot_general(
        eye, grown / jnp.sum(grown, axis=0, keepdims=True), (((1,), (1,)), ((), ())),
        precision=lax.Precision.HIGHEST, preferred_element_type=F32,
    )

    for k in range(1, nz):
        frm = pl.multiple_of(zz(-k) * zb, 16)
        rc(t2.at[pl.ds(0, zb)], fin.at[pl.ds(frm, zb)], us.at[k], ur.at[k]).wait_recv()
    total = weight[:, 0:1] * dot(pick[0].astype(F32).astype(BF), fin[...])
    total += weight[:, 1:2] * dot(pick[1].astype(F32).astype(BF), fin[...])
    moe_ref[...] = total.astype(BF)
    for copy in sent:
        copy.wait_send()


def call(nz, nx, cap, *args):
    rows = nz * nx * cap
    vm = pl.BlockSpec(memory_space=pltpu.VMEM)
    hbm = pl.BlockSpec(memory_space=pltpu.HBM)
    dma = lambda *n: pltpu.SemaphoreType.DMA(n)
    big = lambda *s: pltpu.VMEM(s, BF)
    wide = lambda *s: pltpu.VMEM(s, F32)
    scratch = [
        big(64, 512), big(128, 128), big(128, 128), big(128, 2048), wide(1, 2048), wide(1, 2048),
        big(64, 512), big(128, 128), big(rows, 256), big(rows, rows),
        big(nz, nx, 128, 128), big(4, 64, 512), big(8, 128, 512), wide(8, ODIM, 256), big(8, ODIM, 256),
        big(3, 2, ODIM, 256), big(4, 64, 2048), big(4, 32, 2048), big(3, 32, 2048),
        big(rows, 256), big(rows, 256), big(NY, rows, 256), big(2048, 256), big(2048, 256), big(NY, 256, 256),
        wide(rows, 256), wide(rows, 256), wide(2, rows, 256), wide(NY, rows, 128), big(NY, rows, 128),
        big(NY, rows, 128), big(NY, rows, 128), big(7, rows, 128), big(rows, 128), big(rows, 128),
        big(rows, 128), big(rows, 128),
        dma(17), dma(nx), dma(nx), dma(nz), dma(nz), dma(nz), dma(nz), dma(3), dma(3), dma(3), dma(3), dma(3), dma(3),
        dma(3), dma(3),
        dma(nz), dma(nz), dma(2, nx), dma(2, nx), dma(6), dma(6), dma(8), dma(8), dma(8), dma(8), dma(7), dma(7),
        dma(nx), dma(nx), dma(nz), dma(nz),
    ]
    return pl.pallas_call(
        functools.partial(kernel, nz, nx, cap),
        out_shape=(jax.ShapeDtypeStruct((32, 2048), BF), jax.ShapeDtypeStruct((128, 128), BF)),
        in_specs=[vm] * 6 + [hbm] * 10,
        out_specs=(vm, vm),
        scratch_shapes=scratch,
        compiler_params=pltpu.CompilerParams(
            collective_id=0, has_side_effects=True, vmem_limit_bytes=67043328
        ),
        name="layer",
    )(*args)


def per_device(
    q_in, k_in, v_in, q_gain, k_gain, w_out, post_gain, moe_in, routes, route_logits, pre_gain, w_gate, w_up, w_down
):
    nz, nx = lax.axis_size("z"), lax.axis_size("x")
    count, top = routes.shape
    experts = nz * nx
    cap = max(2, 3 * top * count // (2 * experts))
    i = np.arange(experts * cap, dtype=np.int32)
    src = (i % (nz * cap)) // cap * (nx * cap) + i // (nz * cap) * cap + i % cap
    return call(
        nz, nx, cap, jnp.asarray(angle_table()), q_gain[None, :], k_gain[None, :], routes.T, route_logits.T,
        jnp.asarray(src[None, :]), pre_gain[None, :], post_gain[None, :],
        q_in.T, k_in, v_in, moe_in, w_gate[0], w_up[0], w_down[0], w_out,
    )


def solution(mesh):
    ny = mesh.shape["tp"] // 2
    nz = 8 if mesh.shape["ep"] % 8 == 0 else 2
    finer = Mesh(mesh.devices.reshape(nz, mesh.shape["ep"] // nz, ny, 2), ALL)
    in_specs = (
        P(EP, TP), P(EP, None), P(EP, None), P(), P(), P(TP, None), P(), P(EP, None), P(EP, None), P(EP, None), P(),
        P(EP, None, TP), P(EP, None, TP), P(EP, TP, None),
    )
    return jax.shard_map(
        per_device, mesh=finer, in_specs=in_specs, out_specs=(P(ALL, None), P(EP, TP)), check_vma=False
    )
```

```python
import functools

import jax
import jax.numpy as jnp
import numpy as np
from jax import lax
from jax.experimental import pallas as pl
from jax.experimental.pallas import tpu as pltpu
from jax.sharding import Mesh
from jax.sharding import PartitionSpec as P

GRID_W = 128
EPSILON = 1e-06
ROPE_BASE = 10000.0
EP = ("z", "x")
TP = ("y", "c")
ALL = ("z", "x", "y", "c")
NY = 8
ODIM = 80
MESH = pl.DeviceIdType.MESH
BF = jnp.bfloat16
F32 = jnp.float32


def angle_table():
    lane = np.arange(128)
    inverse = np.float32(ROPE_BASE) ** (-np.arange(16, dtype=np.float32) / np.float32(16))
    angle = (np.arange(GRID_W, dtype=np.float32)[:, None] * inverse[None, lane % 16]).astype(np.float64)
    sign = np.where(lane % 32 < 16, -1.0, 1.0)[None, :]
    return np.where(lane[None, :] < 64, np.cos(angle), sign * np.sin(angle)).astype(np.float32)


def dot(a, b):
    return jnp.dot(a, b, preferred_element_type=F32)


def dot_t(a, b):
    return lax.dot_general(a, b, (((0,), (0,)), ((), ())), preferred_element_type=F32)


def dot_nt(a, b):
    return lax.dot_general(a, b, (((1,), (1,)), ((), ())), preferred_element_type=F32)


def iota(shape, dim):
    return lax.broadcasted_iota(jnp.int32, shape, dim)


def kernel(
    nz, nx, cap,
    tab_ref, qg_ref, kg_ref, rt_ref, lg_ref, src_ref, pre_hbm, post_hbm, q_hbm, k_hbm, v_hbm, x_hbm, wg_hbm, wu_hbm, wd_hbm, wo_hbm,
    out_ref, moe_ref,
    qv, kv, vv, xv, prev, pg_ref, q_ref, kv_ref, og_ref, pb_ref,
    kvb, qb, qd, acc, ob, orx, wob, pa, ra,
    zrx, xsb, xb, wg, wu, wd, ga, up, tmp, own, pbuf, prx, psb, rs, ret, rbk, t2, fin,
    lsem, kxs, kxr, rrs, rrr, rls, rlr, qs, qr, ts, tr, wos, wor, as_, ar,
    zs, zr, xs, xr, ys, yr, ds, dr, es, er, ms, mr, vs, vr, us, ur,
):
    z, x, y, c = (lax.axis_index(n) for n in ALL)
    rows = nz * nx * cap
    zb, xbk = nx * cap, nz * cap
    b = lax.rem(y, 2)
    h = y // 2
    m = b * 2 + c
    ysw = y + 1 - 2 * b
    oc = 1 - c
    sgn = 1 - 2 * c

    def yy(k):
        return lax.rem(y + (k + 2 * NY), NY)

    def zz(k):
        return lax.rem(z + (k + nz), nz)

    def xx(k):
        return lax.rem(x + (k + nx), nx)

    sent = []

    def rc(src, dst, ss, rr, dz=None, dx=None, dy=None, dc=None):
        dev = (z if dz is None else dz, x if dx is None else dx, y if dy is None else dy, c if dc is None else dc)
        return pltpu.make_async_remote_copy(src, dst, ss, rr, device_id=dev, device_id_type=MESH)

    def send(*args, **kw):
        copy = rc(*args, **kw)
        copy.start()
        sent.append(copy)

    def local(src, dst, i):
        copy = pltpu.make_async_copy(src, dst, lsem.at[i])
        copy.start()
        return copy

    ep = z * nx + x
    hl = pl.multiple_of((h // 2) * 128, 128)
    mrow = pl.multiple_of(m * 128, 128)
    lk = local(k_hbm.at[pl.ds(mrow, 128), pl.ds(hl, 128)], kv, 11)
    lv = local(v_hbm.at[pl.ds(mrow, 128), pl.ds(hl, 128)], vv, 12)
    lx = local(x_hbm, xv, 13)
    lq = local(q_hbm, qv, 14)
    lpre = local(pre_hbm, prev, 15)
    lpost = local(post_hbm, pg_ref, 16)
    lwo = local(wo_hbm, wob.at[m], 0)
    lwg = local(wg_hbm, wg, 1)
    lwu = local(wu_hbm, wu, 2)
    lwd = [local(wd_hbm.at[:, k * 256 : (k + 1) * 256], wd.at[k], 3 + k) for k in range(NY)]

    bar = pltpu.get_barrier_semaphore()
    peers = [(zz(k), x, y, c) for k in range(1, nz)]
    peers += [(z, xx(k), y, c) for k in range(1, nx)]
    peers += [(z, x, yy(k), c) for k in (1, -1, 2, -2, 4)]
    peers += [(z, x, y, oc), (z, x, ysw, oc)]
    for peer in peers:
        pl.semaphore_signal(bar, inc=1, device_id=peer, device_id_type=MESH)

    def mixer(j, l):
        i = j - 64
        return ((l < 64) & (i == l)) | ((l >= 64) & (i == ((l - 64) ^ 16)))

    wide_mix = mixer(iota((192, 128), 0), iota((192, 128), 1)).astype(F32).astype(BF)
    sub = lax.rem(h, 2)
    hmix = mixer(iota((128, 128), 0) + (1 - sub) * 64, iota((128, 128), 1)).astype(F32).astype(BF)
    qmix = wide_mix[64:128]
    lane = iota((128, 128), 1)
    row_lane = (lane & 63) < 32
    col_table = tab_ref[...]

    def gains(ref):
        return jnp.dot(
            jnp.broadcast_to(ref[...], (8, 64)), qmix.astype(F32), precision=lax.Precision.HIGHEST,
            preferred_element_type=F32,
        )[0:1]

    def turned(values, gain, r):
        table = jnp.where(row_lane, tab_ref[pl.ds(r, 1), :], col_table) * gain
        scale = lax.rsqrt(jnp.mean(values * values, axis=1, keepdims=True) + EPSILON)
        out = values * scale * table
        return out + pltpu.roll(out, 64, 1)

    kgain = gains(kg_ref)
    lk.wait()
    k128 = turned(dot(kv[...], hmix), kgain, ep * 4 + m)
    kv_ref[0:64] = jnp.where(lane[0:64] < 64, k128[0:64], k128[64:128]).astype(BF)
    lv.wait()
    pick = (iota((64, 128), 1) == iota((64, 128), 0) + 64 * sub).astype(F32).astype(BF)
    kv_ref[64:128] = dot_nt(pick, vv[...]).astype(BF)
    kvb[z, x] = kv_ref[...]

    count = xv.shape[0]
    experts = nz * nx
    lx.wait()
    x32 = xv[...].astype(F32)
    xscale = lax.rsqrt(jnp.mean(x32 * x32, axis=1, keepdims=True) + EPSILON)
    lpre.wait()
    normed = []
    for i in range(2):
        col = pl.multiple_of((yy(4 * i) * 2 + c) * 128, 128)
        normed.append((xv[:, pl.ds(col, 128)].astype(F32) * xscale * prev[:, pl.ds(col, 128)]).astype(BF))
    normed = jnp.concatenate(normed, axis=1)
    eid = iota((count, 128), 1)
    eye = (iota((count, count), 1) == iota((count, count), 0)).astype(F32)
    named = dot_nt(eye.astype(BF), rt_ref[...].astype(F32).astype(BF)).astype(jnp.int32)
    hot = [eid == named[:, i : i + 1] for i in range(2)]
    lower = (iota((count, count), 1) < iota((count, count), 0)).astype(F32).astype(BF)
    rank = dot(lower, (hot[0] | hot[1]).astype(F32).astype(BF)) + (cap * eid).astype(F32)
    place = [jnp.sum(jnp.where(hh, rank, 0.0), axis=1, keepdims=True).astype(jnp.int32) for hh in hot]
    slot = iota((count, rows), 1)
    pick = [slot == pp for pp in place]
    og_ref[...] = dot_t((pick[0] | pick[1]).astype(F32).astype(BF), normed).astype(BF)
    pb_ref[...] = (iota((rows, rows), 0) == src_ref[...]).astype(F32).astype(BF)

    lq.wait()
    q128 = dot_t(qv[...], qmix)
    qgain = gains(qg_ref)
    turned_q = [turned(q128[i * 128 : (i + 1) * 128], qgain, ep * 4 + i).astype(BF) for i in range(4)]
    ordered = [turned_q[i][k * 32 : (k + 1) * 32] for k in range(4) for i in range(4)]
    ordered = jnp.concatenate(ordered, axis=0) * BF(0.125)
    pick_q = (iota((64, 128), 1) == iota((64, 128), 0)).astype(F32).astype(BF)
    q_ref[...] = dot_nt(pick_q, ordered).astype(BF)
    qb[m] = q_ref[...]
    zrow = pl.multiple_of(z * zb, 16)
    zrx[pl.ds(zrow, zb), :] = og_ref[pl.ds(zrow, zb), :]
    pl.semaphore_wait(bar, len(peers))

    for k in range(1, nz):
        to = pl.multiple_of(zz(k) * zb, 16)
        send(og_ref.at[pl.ds(to, zb)], zrx.at[pl.ds(zrow, zb)], zs.at[k], zr.at[k], dz=zz(k))
    for k in range(1, nx):
        send(kv_ref, kvb.at[z, x], kxs.at[k], kxr.at[k], dx=xx(k))
    send(q_ref, qb.at[m], qs.at[0], qr.at[0], dc=oc)
    send(q_ref, qb.at[m], qs.at[1], qr.at[1], dy=ysw)
    send(q_ref, qb.at[m], qs.at[2], qr.at[2], dy=ysw, dc=oc)

    for j in range(8):
        qd[j] = jnp.zeros((128, 512), BF)
        acc[j] = jnp.zeros((ODIM, 256), F32)

    def ring(step, i):
        if step < nz // 2:
            g = kvb.at[zz(-step), xx(i)]
            send(g, g, rrs.at[step, i], rrr.at[step, i], dz=zz(1))
        if step < (nz - 1) // 2:
            g = kvb.at[zz(step), xx(i)]
            send(g, g, rls.at[step, i], rlr.at[step, i], dz=zz(-1))

    def ring_wait(step):
        got = []
        if step < nz // 2:
            got.append(zz(-step - 1))
        if step < (nz - 1) // 2:
            got.append(zz(step + 1))
        for i in range(nx):
            if step < nz // 2:
                g = kvb.at[zz(-step - 1), xx(i)]
                rc(g, g, rrs.at[step, i], rrr.at[step, i]).wait_recv()
            if step < (nz - 1) // 2:
                g = kvb.at[zz(step + 1), xx(i)]
                rc(g, g, rls.at[step, i], rlr.at[step, i]).wait_recv()
            ring(step + 1, i)
        return got

    ring(0, 0)
    for k in range(1, nx):
        rc(kv_ref, kvb.at[z, xx(-k)], kxs.at[k], kxr.at[k]).wait_recv()
        ring(0, nx - k)

    for k in range(1, nz):
        frm = pl.multiple_of(zz(-k) * zb, 16)
        rc(og_ref.at[pl.ds(0, zb)], zrx.at[pl.ds(frm, zb)], zs.at[k], zr.at[k]).wait_recv()
    xsb[...] = dot_t(pb_ref[...], zrx[...]).astype(BF)
    cl = pl.multiple_of(c * 128, 128)
    ocl = pl.multiple_of(oc * 128, 128)
    xrow = pl.multiple_of(x * xbk, 16)
    slots = (yy(0), yy(4))
    for i in range(2):
        xb[slots[i], pl.ds(xrow, xbk), pl.ds(cl, 128)] = xsb[pl.ds(xrow, xbk), i * 128 : (i + 1) * 128]
    for k in range(1, nx):
        to = pl.multiple_of(xx(k) * xbk, 16)
        for i in range(2):
            send(
                xsb.at[pl.ds(to, xbk), pl.ds(i * 128, 128)],
                xb.at[slots[i], pl.ds(xrow, xbk), pl.ds(cl, 128)],
                xs.at[i, k], xr.at[i, k], dx=xx(k),
            )

    rc(q_ref, qb.at[b * 2 + oc], qs.at[0], qr.at[0]).wait_recv()
    rc(q_ref, qb.at[(1 - b) * 2 + c], qs.at[1], qr.at[1]).wait_recv()
    rc(q_ref, qb.at[(1 - b) * 2 + oc], qs.at[2], qr.at[2]).wait_recv()
    for mt in range(4):
        for rp in range(2):
            pair = [qb[2 * rp + i, :, mt * 128 : (mt + 1) * 128] for i in range(2)]
            pair = jnp.concatenate(pair, axis=1)
            qd[mt * 2 + rp, 0:64, 0:256] = pair
            qd[mt * 2 + rp, 64:128, 256:512] = pair

    def attend(zi):
        keys = kvb[zi, :, 0:64, :].reshape(nx * 64, 128)
        vals = [kvb[zi, i, 64:128, :] for i in range(nx)]
        vals = jnp.concatenate(vals, axis=1)
        vals = jnp.concatenate([vals, jnp.ones((ODIM - 64, nx * 128), BF)], axis=0)

        def project(p):
            parts = []
            for i in range(nx):
                parts.append(p[i * 64 : (i + 1) * 64, 0:256])
                parts.append(p[i * 64 : (i + 1) * 64, 256:512])
            return jnp.concatenate(parts, axis=0)

        scores = [dot(keys, qd[0]), dot(keys, qd[1])]
        held = None
        for j in range(8):
            p = project(jnp.exp(scores[j]).astype(BF))
            if j < 6:
                scores.append(dot(keys, qd[j + 2]))
            if held is not None:
                acc[j - 1] += dot(vals, held)
            held = p
        acc[7] += dot(vals, held)

    attend(z)

    for k in range(1, nx):
        frm = pl.multiple_of(xx(-k) * xbk, 16)
        for i in range(2):
            rc(
                xsb.at[pl.ds(0, xbk), pl.ds(i * 128, 128)],
                xb.at[slots[i], pl.ds(frm, xbk), pl.ds(cl, 128)],
                xs.at[i, k], xr.at[i, k],
            ).wait_recv()

    def half(slot, which):
        return xb.at[slot, :, pl.ds(which, 128)]

    plan = ((1, 0), (1, 4), (-1, 0), (-1, 4), (2, 0), (-2, 0))
    for i, (k, r) in enumerate(plan):
        g = half(yy(r), cl)
        send(g, g, ys.at[i], yr.at[i], dy=yy(k))

    def swap(r):
        g = half(yy(r), cl)
        send(g, g, ds.at[r], dr.at[r], dc=oc)

    swap(0)
    swap(4)
    lwo.wait()
    send(wob.at[m], wob.at[m], wos.at[0], wor.at[0], dc=oc)
    send(wob.at[m], wob.at[m], wos.at[1], wor.at[1], dy=ysw)

    def arrive(i):
        k, r = plan[i]
        g = half(yy(r - k), cl)
        rc(g, g, ys.at[i], yr.at[i]).wait_recv()
        swap((r - k + NY) % NY)

    steps = max(nz // 2, (nz - 1) // 2)
    for step in range(max(steps - 2, 0)):
        for zi in ring_wait(step):
            attend(zi)
    for i in range(6):
        arrive(i)
    later = ring_wait(steps - 2) if steps > 1 else []

    lwg.wait()
    lwu.wait()
    for i, r in enumerate((0, 4, 1, 5, 7, 3, 2, 6)):
        s = yy(r)
        g = half(s, ocl)
        rc(g, g, ds.at[r], dr.at[r]).wait_recv()
        w0 = pl.multiple_of(s * 256, 256)
        gd = dot(xb[s], wg[pl.ds(w0, 256), :])
        ud = dot(xb[s], wu[pl.ds(w0, 256), :])
        if i == 0:
            ga[...] = gd
            up[...] = ud
        else:
            ga[...] += gd
            up[...] += ud
    gate = ga[...]
    hid = (gate / (1.0 + jnp.exp(-gate)) * up[...]).astype(BF)
    for copy in lwd:
        copy.wait()
    order = (4, 3, 5, 1, 7, 2, 6, 0)
    for r in order:
        tmp[r % 2] = dot(hid, wd[yy(r)])
        own[r] = tmp[r % 2, :, pl.ds(cl, 128)]
        pbuf[r] = tmp[r % 2, :, pl.ds(ocl, 128)].astype(BF)
        send(pbuf.at[r], prx.at[r], es.at[r], er.at[r], dc=oc)

    def paired(r):
        rc(pbuf.at[r], prx.at[r], es.at[r], er.at[r]).wait_recv()
        return own[r] + prx[r].astype(F32)

    for r, i, dest in ((4, 0, yy(0 - 2 * sgn)), (3, 1, yy(1)), (5, 2, yy(-1)), (1, 3, yy(1)), (7, 4, yy(-1))):
        psb[r] = paired(r).astype(BF)
        send(psb.at[r], rs.at[i], ms.at[i], mr.at[i], dy=dest)

    def got_rs(i):
        rc(psb.at[0], rs.at[i], ms.at[i], mr.at[i]).wait_recv()
        return rs[i].astype(F32)

    other = wob.at[(1 - b) * 2 + c]
    rc(other, other, wos.at[1], wor.at[1]).wait_recv()
    send(other, other, wos.at[2], wor.at[2], dc=oc)
    for zi in later:
        attend(zi)
    far_sum = got_rs(0)
    right = c.astype(F32)
    psb[2] = (paired(2) + got_rs(1) + far_sum * right).astype(BF)
    send(psb.at[2], rs.at[5], ms.at[5], mr.at[5], dy=yy(2))
    psb[6] = (paired(6) + got_rs(2) + far_sum * (1.0 - right)).astype(BF)
    send(psb.at[6], rs.at[6], ms.at[6], mr.at[6], dy=yy(-2))

    for zi in ring_wait(steps - 1):
        attend(zi)
    for j in range(8):
        a = acc[j]
        den = a[64:ODIM]
        hi = den.astype(BF)
        lo = (den - hi.astype(F32)).astype(BF)
        first = lax.broadcasted_iota(jnp.int32, (ODIM - 64, 256), 0) == 0
        ob[j, 0:64] = a[0:64].astype(BF)
        ob[j, 64:ODIM] = jnp.where(first, hi.astype(F32), lo.astype(F32)).astype(BF)
    members = ((0, y, oc, b * 2 + oc), (1, ysw, c, (1 - b) * 2 + c), (2, ysw, oc, (1 - b) * 2 + oc))
    for i, dy, dc, mm in members:
        send(ob.at[pl.ds(2 * mm, 2)], orx.at[i], ts.at[i], tr.at[i], dy=dy, dc=dc)

    ret[...] = (paired(0) + got_rs(3) + got_rs(4) + got_rs(5) + got_rs(6)).astype(BF)
    rbk[pl.ds(xrow, xbk), :] = ret[pl.ds(xrow, xbk), :]
    for k in range(1, nx):
        to = pl.multiple_of(xx(k) * xbk, 16)
        send(ret.at[pl.ds(to, xbk)], rbk.at[pl.ds(xrow, xbk)], vs.at[k], vr.at[k], dx=xx(k))
    for i, dy, dc, mm in members:
        rc(ob.at[pl.ds(0, 2)], orx.at[i], ts.at[i], tr.at[i]).wait_recv()
    heads = []
    for rp in range(2):
        t = ob[2 * m + rp].astype(F32)
        for i in range(3):
            t += orx[i, rp].astype(F32)
        o = (t[0:64] / (t[64:65] + t[65:66])).astype(BF)
        heads += [o[:, 0:128], o[:, 128:256]]
    hot = jnp.concatenate(heads, axis=0)
    partner = wob.at[b * 2 + oc]
    rc(partner, partner, wos.at[0], wor.at[0]).wait_recv()
    far = wob.at[(1 - b) * 2 + oc]
    rc(far, far, wos.at[2], wor.at[2]).wait_recv()
    for n in range(4):
        part = dot_t(hot, wob[:, :, n * 512 : (n + 1) * 512].reshape(256, 512))
        pa[:, :, n * 512 : (n + 1) * 512] = part.astype(BF).reshape(4, 32, 512)

    for k in range(1, 4):
        send(pa.at[lax.rem(h + k, 4)], ra.at[k - 1], as_.at[k - 1], ar.at[k - 1], dy=yy(2 * k))

    for k in range(1, nx):
        frm = pl.multiple_of(xx(-k) * xbk, 16)
        rc(ret.at[pl.ds(0, xbk)], rbk.at[pl.ds(frm, xbk)], vs.at[k], vr.at[k]).wait_recv()
    t2[...] = dot(pb_ref[...], rbk[...]).astype(BF)
    fin[pl.ds(zrow, zb), :] = t2[pl.ds(zrow, zb), :]
    for k in range(1, nz):
        to = pl.multiple_of(zz(k) * zb, 16)
        send(t2.at[pl.ds(to, zb)], fin.at[pl.ds(zrow, zb)], us.at[k], ur.at[k], dz=zz(k))

    mixed = pa[h].astype(F32)
    for k in range(1, 4):
        rc(pa.at[0], ra.at[k - 1], as_.at[k - 1], ar.at[k - 1]).wait_recv()
        mixed += ra[k - 1].astype(F32)
    scale = lax.rsqrt(jnp.mean(mixed * mixed, axis=1, keepdims=True) + EPSILON)
    lpost.wait()
    out_ref[...] = (mixed * scale * pg_ref[...]).astype(BF)

    logits = lg_ref[...]
    grown = jnp.exp(logits - jnp.max(logits, axis=0, keepdims=True))
    weight = lax.dot_general(
        eye, grown / jnp.sum(grown, axis=0, keepdims=True), (((1,), (1,)), ((), ())),
        precision=lax.Precision.HIGHEST, preferred_element_type=F32,
    )

    for k in range(1, nz):
        frm = pl.multiple_of(zz(-k) * zb, 16)
        rc(t2.at[pl.ds(0, zb)], fin.at[pl.ds(frm, zb)], us.at[k], ur.at[k]).wait_recv()
    total = weight[:, 0:1] * dot(pick[0].astype(F32).astype(BF), fin[...])
    total += weight[:, 1:2] * dot(pick[1].astype(F32).astype(BF), fin[...])
    moe_ref[...] = total.astype(BF)
    for copy in sent:
        copy.wait_send()


def call(nz, nx, cap, *args):
    rows = nz * nx * cap
    vm = pl.BlockSpec(memory_space=pltpu.VMEM)
    hbm = pl.BlockSpec(memory_space=pltpu.HBM)
    dma = lambda *n: pltpu.SemaphoreType.DMA(n)
    big = lambda *s: pltpu.VMEM(s, BF)
    wide = lambda *s: pltpu.VMEM(s, F32)
    scratch = [
        big(64, 512), big(128, 128), big(128, 128), big(128, 2048), wide(1, 2048), wide(1, 2048),
        big(64, 512), big(128, 128), big(rows, 256), big(rows, rows),
        big(nz, nx, 128, 128), big(4, 64, 512), big(8, 128, 512), wide(8, ODIM, 256), big(8, ODIM, 256),
        big(3, 2, ODIM, 256), big(4, 64, 2048), big(4, 32, 2048), big(3, 32, 2048),
        big(rows, 256), big(rows, 256), big(NY, rows, 256), big(2048, 256), big(2048, 256), big(NY, 256, 256),
        wide(rows, 256), wide(rows, 256), wide(2, rows, 256), wide(NY, rows, 128), big(NY, rows, 128),
        big(NY, rows, 128), big(NY, rows, 128), big(7, rows, 128), big(rows, 128), big(rows, 128),
        big(rows, 128), big(rows, 128),
        dma(17), dma(nx), dma(nx), dma(nz, nx), dma(nz, nx), dma(nz, nx), dma(nz, nx), dma(3), dma(3), dma(3), dma(3), dma(3), dma(3),
        dma(3), dma(3),
        dma(nz), dma(nz), dma(2, nx), dma(2, nx), dma(6), dma(6), dma(8), dma(8), dma(8), dma(8), dma(7), dma(7),
        dma(nx), dma(nx), dma(nz), dma(nz),
    ]
    return pl.pallas_call(
        functools.partial(kernel, nz, nx, cap),
        out_shape=(jax.ShapeDtypeStruct((32, 2048), BF), jax.ShapeDtypeStruct((128, 128), BF)),
        in_specs=[vm] * 6 + [hbm] * 10,
        out_specs=(vm, vm),
        scratch_shapes=scratch,
        compiler_params=pltpu.CompilerParams(
            collective_id=0, has_side_effects=True, vmem_limit_bytes=67043328 - 200 * 1024
        ),
        name="layer",
    )(*args)


def per_device(
    q_in, k_in, v_in, q_gain, k_gain, w_out, post_gain, moe_in, routes, route_logits, pre_gain, w_gate, w_up, w_down
):
    nz, nx = lax.axis_size("z"), lax.axis_size("x")
    count, top = routes.shape
    experts = nz * nx
    cap = max(2, 3 * top * count // (2 * experts))
    i = np.arange(experts * cap, dtype=np.int32)
    src = (i % (nz * cap)) // cap * (nx * cap) + i // (nz * cap) * cap + i % cap
    return call(
        nz, nx, cap, jnp.asarray(angle_table()), q_gain[None, :], k_gain[None, :], routes.T, route_logits.T,
        jnp.asarray(src[None, :]), pre_gain[None, :], post_gain[None, :],
        q_in.T, k_in, v_in, moe_in, w_gate[0], w_up[0], w_down[0], w_out,
    )


def solution(mesh):
    ny = mesh.shape["tp"] // 2
    nz = 8 if mesh.shape["ep"] % 8 == 0 else 2
    finer = Mesh(mesh.devices.reshape(nz, mesh.shape["ep"] // nz, ny, 2), ALL)
    in_specs = (
        P(EP, TP), P(EP, None), P(EP, None), P(), P(), P(TP, None), P(), P(EP, None), P(EP, None), P(EP, None), P(),
        P(EP, None, TP), P(EP, None, TP), P(EP, TP, None),
    )
    return jax.shard_map(
        per_device, mesh=finer, in_specs=in_specs, out_specs=(P(ALL, None), P(EP, TP)), check_vma=False
    )
```

```python
import functools

import jax
import jax.numpy as jnp
import numpy as np
from jax import lax
from jax.experimental import pallas as pl
from jax.experimental.pallas import tpu as pltpu
from jax.sharding import Mesh
from jax.sharding import PartitionSpec as P

GRID_W = 128
EPSILON = 1e-06
ROPE_BASE = 10000.0
EP = ("z", "x")
TP = ("y", "c")
ALL = ("z", "x", "y", "c")
NY = 8
ODIM = 80
MESH = pl.DeviceIdType.MESH
BF = jnp.bfloat16
F32 = jnp.float32


def angle_table():
    lane = np.arange(128)
    inverse = np.float32(ROPE_BASE) ** (-np.arange(16, dtype=np.float32) / np.float32(16))
    angle = (np.arange(GRID_W, dtype=np.float32)[:, None] * inverse[None, lane % 16]).astype(np.float64)
    sign = np.where(lane % 32 < 16, -1.0, 1.0)[None, :]
    return np.where(lane[None, :] < 64, np.cos(angle), sign * np.sin(angle)).astype(np.float32)


def dot(a, b):
    return jnp.dot(a, b, preferred_element_type=F32)


def dot_t(a, b):
    return lax.dot_general(a, b, (((0,), (0,)), ((), ())), preferred_element_type=F32)


def dot_nt(a, b):
    return lax.dot_general(a, b, (((1,), (1,)), ((), ())), preferred_element_type=F32)


def iota(shape, dim):
    return lax.broadcasted_iota(jnp.int32, shape, dim)


def kernel(
    nz, nx, cap,
    tab_ref, qg_ref, kg_ref, rt_ref, lg_ref, src_ref, pre_hbm, post_hbm, q_hbm, k_hbm, v_hbm, x_hbm, wg_hbm, wu_hbm, wd_hbm, wo_hbm,
    out_ref, moe_ref,
    qv, kv, vv, xv, prev, pg_ref, q_ref, kv_ref, og_ref, pb_ref,
    kvb, qb, qd, acc, ob, orx, wall, ho, hb,
    zrx, xsb, xb, wg, wu, wd, ga, up, tmp, own, pbuf, prx, psb, rs, ret, rbk, t2, fin,
    lsem, kxs, kxr, rrs, rrr, rls, rlr, qs, qr, ts, tr, wys, wyr, wxs, wxr, wds, wdr, as_, ar,
    zs, zr, xs, xr, ys, yr, ds, dr, es, er, ms, mr, vs, vr, us, ur,
):
    z, x, y, c = (lax.axis_index(n) for n in ALL)
    rows = nz * nx * cap
    zb, xbk = nx * cap, nz * cap
    b = lax.rem(y, 2)
    h = y // 2
    m = b * 2 + c
    ysw = y + 1 - 2 * b
    oc = 1 - c
    sgn = 1 - 2 * c

    def yy(k):
        return lax.rem(y + (k + 2 * NY), NY)

    def zz(k):
        return lax.rem(z + (k + nz), nz)

    def xx(k):
        return lax.rem(x + (k + nx), nx)

    sent = []

    def rc(src, dst, ss, rr, dz=None, dx=None, dy=None, dc=None):
        dev = (z if dz is None else dz, x if dx is None else dx, y if dy is None else dy, c if dc is None else dc)
        return pltpu.make_async_remote_copy(src, dst, ss, rr, device_id=dev, device_id_type=MESH)

    def send(*args, **kw):
        copy = rc(*args, **kw)
        copy.start()
        sent.append(copy)

    def local(src, dst, i):
        copy = pltpu.make_async_copy(src, dst, lsem.at[i])
        copy.start()
        return copy

    ep = z * nx + x
    hl = pl.multiple_of((h // 2) * 128, 128)
    mrow = pl.multiple_of(m * 128, 128)
    lk = local(k_hbm.at[pl.ds(mrow, 128), pl.ds(hl, 128)], kv, 11)
    lv = local(v_hbm.at[pl.ds(mrow, 128), pl.ds(hl, 128)], vv, 12)
    lx = local(x_hbm, xv, 13)
    lq = local(q_hbm, qv, 14)
    lpre = local(pre_hbm, prev, 15)
    lpost = local(post_hbm, pg_ref, 16)
    wc = 2048 // nx
    lwo = local(wo_hbm.at[:, pl.ds(pl.multiple_of(x * wc, 128), wc)], wall.at[x, c, y], 0)
    lwg = local(wg_hbm, wg, 1)
    lwu = local(wu_hbm, wu, 2)
    lwd = [local(wd_hbm.at[:, k * 256 : (k + 1) * 256], wd.at[k], 3 + k) for k in range(NY)]

    bar = pltpu.get_barrier_semaphore()
    peers = [(zz(k), x, y, c) for k in range(1, nz)]
    peers += [(z, xx(k), y, c) for k in range(1, nx)]
    peers += [(z, x, yy(k), c) for k in (1, -1, 2, -2, 3, -3, 4)]
    peers += [(z, x, y, oc), (z, x, ysw, oc)]
    for peer in peers:
        pl.semaphore_signal(bar, inc=1, device_id=peer, device_id_type=MESH)

    def mixer(j, l):
        i = j - 64
        return ((l < 64) & (i == l)) | ((l >= 64) & (i == ((l - 64) ^ 16)))

    wide_mix = mixer(iota((192, 128), 0), iota((192, 128), 1)).astype(F32).astype(BF)
    sub = lax.rem(h, 2)
    hmix = mixer(iota((128, 128), 0) + (1 - sub) * 64, iota((128, 128), 1)).astype(F32).astype(BF)
    qmix = wide_mix[64:128]
    lane = iota((128, 128), 1)
    row_lane = (lane & 63) < 32
    col_table = tab_ref[...]

    def gains(ref):
        return jnp.dot(
            jnp.broadcast_to(ref[...], (8, 64)), qmix.astype(F32), precision=lax.Precision.HIGHEST,
            preferred_element_type=F32,
        )[0:1]

    def turned(values, gain, r):
        table = jnp.where(row_lane, tab_ref[pl.ds(r, 1), :], col_table) * gain
        scale = lax.rsqrt(jnp.mean(values * values, axis=1, keepdims=True) + EPSILON)
        out = values * scale * table
        return out + pltpu.roll(out, 64, 1)

    kgain = gains(kg_ref)
    lk.wait()
    k128 = turned(dot(kv[...], hmix), kgain, ep * 4 + m)
    kv_ref[0:64] = jnp.where(lane[0:64] < 64, k128[0:64], k128[64:128]).astype(BF)
    lv.wait()
    pick = (iota((64, 128), 1) == iota((64, 128), 0) + 64 * sub).astype(F32).astype(BF)
    kv_ref[64:128] = dot_nt(pick, vv[...]).astype(BF)
    kvb[z, x] = kv_ref[...]

    count = xv.shape[0]
    experts = nz * nx
    lx.wait()
    x32 = xv[...].astype(F32)
    xscale = lax.rsqrt(jnp.mean(x32 * x32, axis=1, keepdims=True) + EPSILON)
    lpre.wait()
    normed = []
    for i in range(2):
        col = pl.multiple_of((yy(4 * i) * 2 + c) * 128, 128)
        normed.append((xv[:, pl.ds(col, 128)].astype(F32) * xscale * prev[:, pl.ds(col, 128)]).astype(BF))
    normed = jnp.concatenate(normed, axis=1)
    eid = iota((count, 128), 1)
    eye = (iota((count, count), 1) == iota((count, count), 0)).astype(F32)
    named = dot_nt(eye.astype(BF), rt_ref[...].astype(F32).astype(BF)).astype(jnp.int32)
    hot = [eid == named[:, i : i + 1] for i in range(2)]
    lower = (iota((count, count), 1) < iota((count, count), 0)).astype(F32).astype(BF)
    rank = dot(lower, (hot[0] | hot[1]).astype(F32).astype(BF)) + (cap * eid).astype(F32)
    place = [jnp.sum(jnp.where(hh, rank, 0.0), axis=1, keepdims=True).astype(jnp.int32) for hh in hot]
    slot = iota((count, rows), 1)
    pick = [slot == pp for pp in place]
    og_ref[...] = dot_t((pick[0] | pick[1]).astype(F32).astype(BF), normed).astype(BF)
    pb_ref[...] = (iota((rows, rows), 0) == src_ref[...]).astype(F32).astype(BF)

    lq.wait()
    q128 = dot_t(qv[...], qmix)
    qgain = gains(qg_ref)
    turned_q = [turned(q128[i * 128 : (i + 1) * 128], qgain, ep * 4 + i).astype(BF) for i in range(4)]
    ordered = [turned_q[i][k * 32 : (k + 1) * 32] for k in range(4) for i in range(4)]
    ordered = jnp.concatenate(ordered, axis=0) * BF(0.125)
    pick_q = (iota((64, 128), 1) == iota((64, 128), 0)).astype(F32).astype(BF)
    q_ref[...] = dot_nt(pick_q, ordered).astype(BF)
    qb[m] = q_ref[...]
    zrow = pl.multiple_of(z * zb, 16)
    zrx[pl.ds(zrow, zb), :] = og_ref[pl.ds(zrow, zb), :]
    pl.semaphore_wait(bar, len(peers))

    for k in range(1, nz):
        to = pl.multiple_of(zz(k) * zb, 16)
        send(og_ref.at[pl.ds(to, zb)], zrx.at[pl.ds(zrow, zb)], zs.at[k], zr.at[k], dz=zz(k))
    for k in range(1, nx):
        send(kv_ref, kvb.at[z, x], kxs.at[k], kxr.at[k], dx=xx(k))
    send(q_ref, qb.at[m], qs.at[0], qr.at[0], dc=oc)
    send(q_ref, qb.at[m], qs.at[1], qr.at[1], dy=ysw)
    send(q_ref, qb.at[m], qs.at[2], qr.at[2], dy=ysw, dc=oc)

    lwo.wait()
    for k in (1, 7, 2, 6, 3, 5, 4):
        send(wall.at[x, c, y], wall.at[x, c, y], wys.at[k], wyr.at[k], dy=yy(k))

    for j in range(8):
        qd[j] = jnp.zeros((128, 512), BF)
        acc[j] = jnp.zeros((ODIM, 256), F32)

    def ring(step, i):
        if step < nz // 2:
            g = kvb.at[zz(-step), xx(i)]
            send(g, g, rrs.at[step, i], rrr.at[step, i], dz=zz(1))
        if step < (nz - 1) // 2:
            g = kvb.at[zz(step), xx(i)]
            send(g, g, rls.at[step, i], rlr.at[step, i], dz=zz(-1))

    def ring_wait(step):
        got = []
        if step < nz // 2:
            got.append(zz(-step - 1))
        if step < (nz - 1) // 2:
            got.append(zz(step + 1))
        for i in range(nx):
            if step < nz // 2:
                g = kvb.at[zz(-step - 1), xx(i)]
                rc(g, g, rrs.at[step, i], rrr.at[step, i]).wait_recv()
            if step < (nz - 1) // 2:
                g = kvb.at[zz(step + 1), xx(i)]
                rc(g, g, rls.at[step, i], rlr.at[step, i]).wait_recv()
            ring(step + 1, i)
        return got

    ring(0, 0)
    for k in range(1, nx):
        rc(kv_ref, kvb.at[z, xx(-k)], kxs.at[k], kxr.at[k]).wait_recv()
        ring(0, nx - k)

    for k in range(1, nz):
        frm = pl.multiple_of(zz(-k) * zb, 16)
        rc(og_ref.at[pl.ds(0, zb)], zrx.at[pl.ds(frm, zb)], zs.at[k], zr.at[k]).wait_recv()
    xsb[...] = dot_t(pb_ref[...], zrx[...]).astype(BF)
    cl = pl.multiple_of(c * 128, 128)
    ocl = pl.multiple_of(oc * 128, 128)
    xrow = pl.multiple_of(x * xbk, 16)
    slots = (yy(0), yy(4))
    for i in range(2):
        xb[slots[i], pl.ds(xrow, xbk), pl.ds(cl, 128)] = xsb[pl.ds(xrow, xbk), i * 128 : (i + 1) * 128]
    for k in range(1, nx):
        to = pl.multiple_of(xx(k) * xbk, 16)
        for i in range(2):
            send(
                xsb.at[pl.ds(to, xbk), pl.ds(i * 128, 128)],
                xb.at[slots[i], pl.ds(xrow, xbk), pl.ds(cl, 128)],
                xs.at[i, k], xr.at[i, k], dx=xx(k),
            )

    rc(q_ref, qb.at[b * 2 + oc], qs.at[0], qr.at[0]).wait_recv()
    rc(q_ref, qb.at[(1 - b) * 2 + c], qs.at[1], qr.at[1]).wait_recv()
    rc(q_ref, qb.at[(1 - b) * 2 + oc], qs.at[2], qr.at[2]).wait_recv()
    for mt in range(4):
        for rp in range(2):
            pair = [qb[2 * rp + i, :, mt * 128 : (mt + 1) * 128] for i in range(2)]
            pair = jnp.concatenate(pair, axis=1)
            qd[mt * 2 + rp, 0:64, 0:256] = pair
            qd[mt * 2 + rp, 64:128, 256:512] = pair

    def attend(zi):
        keys = kvb[zi, :, 0:64, :].reshape(nx * 64, 128)
        vals = [kvb[zi, i, 64:128, :] for i in range(nx)]
        vals = jnp.concatenate(vals, axis=1)
        vals = jnp.concatenate([vals, jnp.ones((ODIM - 64, nx * 128), BF)], axis=0)

        def project(p):
            parts = []
            for i in range(nx):
                parts.append(p[i * 64 : (i + 1) * 64, 0:256])
                parts.append(p[i * 64 : (i + 1) * 64, 256:512])
            return jnp.concatenate(parts, axis=0)

        scores = [dot(keys, qd[0]), dot(keys, qd[1])]
        held = None
        for j in range(8):
            p = project(jnp.exp(scores[j]).astype(BF))
            if j < 6:
                scores.append(dot(keys, qd[j + 2]))
            if held is not None:
                acc[j - 1] += dot(vals, held)
            held = p
        acc[7] += dot(vals, held)

    attend(z)

    for k in range(1, nx):
        frm = pl.multiple_of(xx(-k) * xbk, 16)
        for i in range(2):
            rc(
                xsb.at[pl.ds(0, xbk), pl.ds(i * 128, 128)],
                xb.at[slots[i], pl.ds(frm, xbk), pl.ds(cl, 128)],
                xs.at[i, k], xr.at[i, k],
            ).wait_recv()

    def half(slot, which):
        return xb.at[slot, :, pl.ds(which, 128)]

    plan = ((1, 0), (1, 4), (-1, 0), (-1, 4), (2, 0), (-2, 0))
    for i, (k, r) in enumerate(plan):
        g = half(yy(r), cl)
        send(g, g, ys.at[i], yr.at[i], dy=yy(k))

    def swap(r):
        g = half(yy(r), cl)
        send(g, g, ds.at[r], dr.at[r], dc=oc)

    swap(0)
    swap(4)
    for k in range(1, NY):
        g = wall.at[x, c, yy(-k)]
        rc(g, g, wys.at[k], wyr.at[k]).wait_recv()
    for k in range(1, nx):
        send(wall.at[x, c], wall.at[x, c], wxs.at[k], wxr.at[k], dx=xx(k))
    send(wall.at[x, c], wall.at[x, c], wds.at[0], wdr.at[0], dc=oc)

    def arrive(i):
        k, r = plan[i]
        g = half(yy(r - k), cl)
        rc(g, g, ys.at[i], yr.at[i]).wait_recv()
        swap((r - k + NY) % NY)

    steps = max(nz // 2, (nz - 1) // 2)
    for step in range(max(steps - 2, 0)):
        for zi in ring_wait(step):
            attend(zi)
    for i in range(6):
        arrive(i)
    later = ring_wait(steps - 2) if steps > 1 else []

    lwg.wait()
    lwu.wait()
    for i, r in enumerate((0, 4, 1, 5, 7, 3, 2, 6)):
        s = yy(r)
        g = half(s, ocl)
        rc(g, g, ds.at[r], dr.at[r]).wait_recv()
        w0 = pl.multiple_of(s * 256, 256)
        gd = dot(xb[s], wg[pl.ds(w0, 256), :])
        ud = dot(xb[s], wu[pl.ds(w0, 256), :])
        if i == 0:
            ga[...] = gd
            up[...] = ud
        else:
            ga[...] += gd
            up[...] += ud
    gate = ga[...]
    hid = (gate / (1.0 + jnp.exp(-gate)) * up[...]).astype(BF)
    for copy in lwd:
        copy.wait()
    order = (4, 3, 5, 1, 7, 2, 6, 0)
    for r in order:
        tmp[r % 2] = dot(hid, wd[yy(r)])
        own[r] = tmp[r % 2, :, pl.ds(cl, 128)]
        pbuf[r] = tmp[r % 2, :, pl.ds(ocl, 128)].astype(BF)
        send(pbuf.at[r], prx.at[r], es.at[r], er.at[r], dc=oc)

    def paired(r):
        rc(pbuf.at[r], prx.at[r], es.at[r], er.at[r]).wait_recv()
        return own[r] + prx[r].astype(F32)

    for r, i, dest in ((4, 0, yy(0 - 2 * sgn)), (3, 1, yy(1)), (5, 2, yy(-1)), (1, 3, yy(1)), (7, 4, yy(-1))):
        psb[r] = paired(r).astype(BF)
        send(psb.at[r], rs.at[i], ms.at[i], mr.at[i], dy=dest)

    def got_rs(i):
        rc(psb.at[0], rs.at[i], ms.at[i], mr.at[i]).wait_recv()
        return rs[i].astype(F32)

    for zi in later:
        attend(zi)
    for k in range(1, nx):
        g = wall.at[xx(-k), c]
        rc(g, g, wxs.at[k], wxr.at[k]).wait_recv()
        send(g, g, wds.at[k], wdr.at[k], dc=oc)
    far_sum = got_rs(0)
    right = c.astype(F32)
    psb[2] = (paired(2) + got_rs(1) + far_sum * right).astype(BF)
    send(psb.at[2], rs.at[5], ms.at[5], mr.at[5], dy=yy(2))
    psb[6] = (paired(6) + got_rs(2) + far_sum * (1.0 - right)).astype(BF)
    send(psb.at[6], rs.at[6], ms.at[6], mr.at[6], dy=yy(-2))

    for zi in ring_wait(steps - 1):
        attend(zi)
    for j in range(8):
        a = acc[j]
        den = a[64:ODIM]
        hi = den.astype(BF)
        lo = (den - hi.astype(F32)).astype(BF)
        first = lax.broadcasted_iota(jnp.int32, (ODIM - 64, 256), 0) == 0
        ob[j, 0:64] = a[0:64].astype(BF)
        ob[j, 64:ODIM] = jnp.where(first, hi.astype(F32), lo.astype(F32)).astype(BF)
    members = ((0, y, oc, b * 2 + oc), (1, ysw, c, (1 - b) * 2 + c), (2, ysw, oc, (1 - b) * 2 + oc))
    for i, dy, dc, mm in members:
        send(ob.at[pl.ds(2 * mm, 2)], orx.at[i], ts.at[i], tr.at[i], dy=dy, dc=dc)

    ret[...] = (paired(0) + got_rs(3) + got_rs(4) + got_rs(5) + got_rs(6)).astype(BF)
    rbk[pl.ds(xrow, xbk), :] = ret[pl.ds(xrow, xbk), :]
    for k in range(1, nx):
        to = pl.multiple_of(xx(k) * xbk, 16)
        send(ret.at[pl.ds(to, xbk)], rbk.at[pl.ds(xrow, xbk)], vs.at[k], vr.at[k], dx=xx(k))
    for i, dy, dc, mm in members:
        rc(ob.at[pl.ds(0, 2)], orx.at[i], ts.at[i], tr.at[i]).wait_recv()
    heads = []
    for rp in range(2):
        t = ob[2 * m + rp].astype(F32)
        for i in range(3):
            t += orx[i, rp].astype(F32)
        o = (t[0:64] / (t[64:65] + t[65:66])).astype(BF)
        heads += [o[:, 0:128], o[:, 128:256]]
    heads = jnp.concatenate(heads, axis=0)
    square = (iota((256, 256), 0) == iota((256, 256), 1)).astype(F32).astype(BF)
    ho[...] = dot_t(heads, square).astype(BF).reshape(4, 32, 256)
    hb[h] = ho[h]
    for k in range(1, 4):
        send(ho.at[lax.rem(h + k, 4)], hb.at[h], as_.at[k - 1], ar.at[k - 1], dy=yy(2 * k))

    for k in range(1, nx):
        frm = pl.multiple_of(xx(-k) * xbk, 16)
        rc(ret.at[pl.ds(0, xbk)], rbk.at[pl.ds(frm, xbk)], vs.at[k], vr.at[k]).wait_recv()
    t2[...] = dot(pb_ref[...], rbk[...]).astype(BF)
    fin[pl.ds(zrow, zb), :] = t2[pl.ds(zrow, zb), :]
    for k in range(1, nz):
        to = pl.multiple_of(zz(k) * zb, 16)
        send(t2.at[pl.ds(to, zb)], fin.at[pl.ds(zrow, zb)], us.at[k], ur.at[k], dz=zz(k))

    for k in range(1, nx):
        g = wall.at[xx(-k), oc]
        rc(g, g, wds.at[k], wdr.at[k]).wait_recv()
    rc(wall.at[x, oc], wall.at[x, oc], wds.at[0], wdr.at[0]).wait_recv()
    for k in range(1, 4):
        rc(ho.at[0], hb.at[lax.rem(h - k + 4, 4)], as_.at[k - 1], ar.at[k - 1]).wait_recv()
    columns = []
    for n in range(nx):
        part = None
        for g in range(4):
            w = jnp.concatenate([wall[n, r % 2, 2 * g + r // 2] for r in range(4)], axis=0)
            part = dot(hb[g], w) if part is None else part + dot(hb[g], w)
        columns.append(part)
    mixed = jnp.concatenate(columns, axis=1)
    scale = lax.rsqrt(jnp.mean(mixed * mixed, axis=1, keepdims=True) + EPSILON)
    lpost.wait()
    out_ref[...] = (mixed * scale * pg_ref[...]).astype(BF)

    logits = lg_ref[...]
    grown = jnp.exp(logits - jnp.max(logits, axis=0, keepdims=True))
    weight = lax.dot_general(
        eye, grown / jnp.sum(grown, axis=0, keepdims=True), (((1,), (1,)), ((), ())),
        precision=lax.Precision.HIGHEST, preferred_element_type=F32,
    )

    for k in range(1, nz):
        frm = pl.multiple_of(zz(-k) * zb, 16)
        rc(t2.at[pl.ds(0, zb)], fin.at[pl.ds(frm, zb)], us.at[k], ur.at[k]).wait_recv()
    total = weight[:, 0:1] * dot(pick[0].astype(F32).astype(BF), fin[...])
    total += weight[:, 1:2] * dot(pick[1].astype(F32).astype(BF), fin[...])
    moe_ref[...] = total.astype(BF)
    for copy in sent:
        copy.wait_send()


def call(nz, nx, cap, *args):
    rows = nz * nx * cap
    vm = pl.BlockSpec(memory_space=pltpu.VMEM)
    hbm = pl.BlockSpec(memory_space=pltpu.HBM)
    dma = lambda *n: pltpu.SemaphoreType.DMA(n)
    big = lambda *s: pltpu.VMEM(s, BF)
    wide = lambda *s: pltpu.VMEM(s, F32)
    scratch = [
        big(64, 512), big(128, 128), big(128, 128), big(128, 2048), wide(1, 2048), wide(1, 2048),
        big(64, 512), big(128, 128), big(rows, 256), big(rows, rows),
        big(nz, nx, 128, 128), big(4, 64, 512), big(8, 128, 512), wide(8, ODIM, 256), big(8, ODIM, 256),
        big(3, 2, ODIM, 256), big(nx, 2, NY, 64, 2048 // nx), big(4, 32, 256), big(4, 32, 256),
        big(rows, 256), big(rows, 256), big(NY, rows, 256), big(2048, 256), big(2048, 256), big(NY, 256, 256),
        wide(rows, 256), wide(rows, 256), wide(2, rows, 256), wide(NY, rows, 128), big(NY, rows, 128),
        big(NY, rows, 128), big(NY, rows, 128), big(7, rows, 128), big(rows, 128), big(rows, 128),
        big(rows, 128), big(rows, 128),
        dma(17), dma(nx), dma(nx), dma(nz, nx), dma(nz, nx), dma(nz, nx), dma(nz, nx), dma(3), dma(3), dma(3), dma(3), dma(NY), dma(NY), dma(nx), dma(nx),
        dma(nx), dma(nx), dma(3), dma(3),
        dma(nz), dma(nz), dma(2, nx), dma(2, nx), dma(6), dma(6), dma(8), dma(8), dma(8), dma(8), dma(7), dma(7),
        dma(nx), dma(nx), dma(nz), dma(nz),
    ]
    return pl.pallas_call(
        functools.partial(kernel, nz, nx, cap),
        out_shape=(jax.ShapeDtypeStruct((32, 2048), BF), jax.ShapeDtypeStruct((128, 128), BF)),
        in_specs=[vm] * 6 + [hbm] * 10,
        out_specs=(vm, vm),
        scratch_shapes=scratch,
        compiler_params=pltpu.CompilerParams(
            collective_id=0, has_side_effects=True, vmem_limit_bytes=67043328 - 200 * 1024
        ),
        name="layer",
    )(*args)


def per_device(
    q_in, k_in, v_in, q_gain, k_gain, w_out, post_gain, moe_in, routes, route_logits, pre_gain, w_gate, w_up, w_down
):
    nz, nx = lax.axis_size("z"), lax.axis_size("x")
    count, top = routes.shape
    experts = nz * nx
    cap = max(2, 3 * top * count // (2 * experts))
    i = np.arange(experts * cap, dtype=np.int32)
    src = (i % (nz * cap)) // cap * (nx * cap) + i // (nz * cap) * cap + i % cap
    return call(
        nz, nx, cap, jnp.asarray(angle_table()), q_gain[None, :], k_gain[None, :], routes.T, route_logits.T,
        jnp.asarray(src[None, :]), pre_gain[None, :], post_gain[None, :],
        q_in.T, k_in, v_in, moe_in, w_gate[0], w_up[0], w_down[0], w_out,
    )


def solution(mesh):
    ny = mesh.shape["tp"] // 2
    nz = 8 if mesh.shape["ep"] % 8 == 0 else 2
    finer = Mesh(mesh.devices.reshape(nz, mesh.shape["ep"] // nz, ny, 2), ALL)
    in_specs = (
        P(EP, TP), P(EP, None), P(EP, None), P(), P(), P(TP, None), P(), P(EP, None), P(EP, None), P(EP, None), P(),
        P(EP, None, TP), P(EP, None, TP), P(EP, TP, None),
    )
    return jax.shard_map(
        per_device, mesh=finer, in_specs=in_specs, out_specs=(P(ALL, None), P(EP, TP)), check_vma=False
    )
```

```python
import functools

import jax
import jax.numpy as jnp
import numpy as np
from jax import lax
from jax.experimental import pallas as pl
from jax.experimental.pallas import tpu as pltpu
from jax.sharding import Mesh
from jax.sharding import PartitionSpec as P

GRID_W = 128
EPSILON = 1e-06
ROPE_BASE = 10000.0
EP = ("z", "x")
TP = ("y", "c")
ALL = ("z", "x", "y", "c")
NY = 8
ODIM = 80
MESH = pl.DeviceIdType.MESH
BF = jnp.bfloat16
F32 = jnp.float32


def angle_table():
    lane = np.arange(128)
    inverse = np.float32(ROPE_BASE) ** (-np.arange(16, dtype=np.float32) / np.float32(16))
    angle = (np.arange(GRID_W, dtype=np.float32)[:, None] * inverse[None, lane % 16]).astype(np.float64)
    sign = np.where(lane % 32 < 16, -1.0, 1.0)[None, :]
    return np.where(lane[None, :] < 64, np.cos(angle), sign * np.sin(angle)).astype(np.float32)


def dot(a, b):
    return jnp.dot(a, b, preferred_element_type=F32)


def dot_t(a, b):
    return lax.dot_general(a, b, (((0,), (0,)), ((), ())), preferred_element_type=F32)


def dot_nt(a, b):
    return lax.dot_general(a, b, (((1,), (1,)), ((), ())), preferred_element_type=F32)


def iota(shape, dim):
    return lax.broadcasted_iota(jnp.int32, shape, dim)


def kernel(
    nz, nx, cap,
    tab_ref, qg_ref, kg_ref, rt_ref, lg_ref, src_ref, pre_hbm, post_hbm, q_hbm, k_hbm, v_hbm, x_hbm, wg_hbm, wu_hbm, wd_hbm, wo_hbm,
    out_ref, moe_ref,
    qv, kv, vv, xv, prev, pg_ref, q_ref, kv_ref, og_ref, pb_ref,
    kvb, qb, qd, acc, ob, orx, wall, ho, hb,
    zrx, xsb, xb, wg, wu, wd, ga, up, tmp, own, pbuf, prx, psb, rs, ret, rbk, t2, fin,
    lsem, kxs, kxr, rrs, rrr, rls, rlr, qs, qr, ts, tr, wys, wyr, wxs, wxr, wds, wdr, as_, ar,
    zs, zr, xs, xr, ys, yr, ds, dr, es, er, ms, mr, vs, vr, us, ur,
):
    z, x, y, c = (lax.axis_index(n) for n in ALL)
    rows = nz * nx * cap
    zb, xbk = nx * cap, nz * cap
    b = lax.rem(y, 2)
    h = y // 2
    m = b * 2 + c
    ysw = y + 1 - 2 * b
    oc = 1 - c
    sgn = 1 - 2 * c

    def yy(k):
        return lax.rem(y + (k + 2 * NY), NY)

    def zz(k):
        return lax.rem(z + (k + nz), nz)

    def xx(k):
        return lax.rem(x + (k + nx), nx)

    sent = []

    def rc(src, dst, ss, rr, dz=None, dx=None, dy=None, dc=None):
        dev = (z if dz is None else dz, x if dx is None else dx, y if dy is None else dy, c if dc is None else dc)
        return pltpu.make_async_remote_copy(src, dst, ss, rr, device_id=dev, device_id_type=MESH)

    def send(*args, **kw):
        copy = rc(*args, **kw)
        copy.start()
        sent.append(copy)

    def local(src, dst, i):
        copy = pltpu.make_async_copy(src, dst, lsem.at[i])
        copy.start()
        return copy

    ep = z * nx + x
    hl = pl.multiple_of((h // 2) * 128, 128)
    mrow = pl.multiple_of(m * 128, 128)
    lk = local(k_hbm.at[pl.ds(mrow, 128), pl.ds(hl, 128)], kv, 11)
    lv = local(v_hbm.at[pl.ds(mrow, 128), pl.ds(hl, 128)], vv, 12)
    lx = local(x_hbm, xv, 13)
    lq = local(q_hbm, qv, 14)
    lpre = local(pre_hbm, prev, 15)
    lpost = local(post_hbm, pg_ref, 16)
    wc = 2048 // nx
    lwo = local(wo_hbm.at[:, pl.ds(pl.multiple_of(x * wc, 128), wc)], wall.at[x, c, y], 0)
    lwg = local(wg_hbm, wg, 1)
    lwu = local(wu_hbm, wu, 2)
    lwd = [local(wd_hbm.at[:, k * 256 : (k + 1) * 256], wd.at[k], 3 + k) for k in range(NY)]

    bar = pltpu.get_barrier_semaphore()
    peers = [(zz(k), x, y, c) for k in range(1, nz)]
    peers += [(z, xx(k), y, c) for k in range(1, nx)]
    peers += [(z, x, yy(k), c) for k in (1, -1, 2, -2, 3, -3, 4)]
    peers += [(z, x, y, oc), (z, x, ysw, oc)]
    for peer in peers:
        pl.semaphore_signal(bar, inc=1, device_id=peer, device_id_type=MESH)

    def mixer(j, l):
        i = j - 64
        return ((l < 64) & (i == l)) | ((l >= 64) & (i == ((l - 64) ^ 16)))

    wide_mix = mixer(iota((192, 128), 0), iota((192, 128), 1)).astype(F32).astype(BF)
    sub = lax.rem(h, 2)
    hmix = mixer(iota((128, 128), 0) + (1 - sub) * 64, iota((128, 128), 1)).astype(F32).astype(BF)
    qmix = wide_mix[64:128]
    lane = iota((128, 128), 1)
    row_lane = (lane & 63) < 32
    col_table = tab_ref[...]

    def gains(ref):
        return jnp.dot(
            jnp.broadcast_to(ref[...], (8, 64)), qmix.astype(F32), precision=lax.Precision.HIGHEST,
            preferred_element_type=F32,
        )[0:1]

    def turned(values, gain, r):
        table = jnp.where(row_lane, tab_ref[pl.ds(r, 1), :], col_table) * gain
        scale = lax.rsqrt(jnp.mean(values * values, axis=1, keepdims=True) + EPSILON)
        out = values * scale * table
        return out + pltpu.roll(out, 64, 1)

    kgain = gains(kg_ref)
    lk.wait()
    k128 = turned(dot(kv[...], hmix), kgain, ep * 4 + m)
    kv_ref[0:64] = jnp.where(lane[0:64] < 64, k128[0:64], k128[64:128]).astype(BF)
    lv.wait()
    pick = (iota((64, 128), 1) == iota((64, 128), 0) + 64 * sub).astype(F32).astype(BF)
    kv_ref[64:128] = dot_nt(pick, vv[...]).astype(BF)
    kvb[z, x] = kv_ref[...]

    count = xv.shape[0]
    experts = nz * nx
    lx.wait()
    x32 = xv[...].astype(F32)
    xscale = lax.rsqrt(jnp.mean(x32 * x32, axis=1, keepdims=True) + EPSILON)
    lpre.wait()
    normed = []
    for i in range(2):
        col = pl.multiple_of((yy(4 * i) * 2 + c) * 128, 128)
        normed.append((xv[:, pl.ds(col, 128)].astype(F32) * xscale * prev[:, pl.ds(col, 128)]).astype(BF))
    normed = jnp.concatenate(normed, axis=1)
    eid = iota((count, 128), 1)
    eye = (iota((count, count), 1) == iota((count, count), 0)).astype(F32)
    named = dot_nt(eye.astype(BF), rt_ref[...].astype(F32).astype(BF)).astype(jnp.int32)
    hot = [eid == named[:, i : i + 1] for i in range(2)]
    lower = (iota((count, count), 1) < iota((count, count), 0)).astype(F32).astype(BF)
    rank = dot(lower, (hot[0] | hot[1]).astype(F32).astype(BF)) + (cap * eid).astype(F32)
    place = [jnp.sum(jnp.where(hh, rank, 0.0), axis=1, keepdims=True).astype(jnp.int32) for hh in hot]
    slot = iota((count, rows), 1)
    pick = [slot == pp for pp in place]
    og_ref[...] = dot_t((pick[0] | pick[1]).astype(F32).astype(BF), normed).astype(BF)
    pb_ref[...] = (iota((rows, rows), 0) == src_ref[...]).astype(F32).astype(BF)

    lq.wait()
    q128 = dot_t(qv[...], qmix)
    qgain = gains(qg_ref)
    turned_q = [turned(q128[i * 128 : (i + 1) * 128], qgain, ep * 4 + i).astype(BF) for i in range(4)]
    ordered = [turned_q[i][k * 32 : (k + 1) * 32] for k in range(4) for i in range(4)]
    ordered = jnp.concatenate(ordered, axis=0) * BF(0.125)
    pick_q = (iota((64, 128), 1) == iota((64, 128), 0)).astype(F32).astype(BF)
    q_ref[...] = dot_nt(pick_q, ordered).astype(BF)
    qb[m] = q_ref[...]
    zrow = pl.multiple_of(z * zb, 16)
    zrx[pl.ds(zrow, zb), :] = og_ref[pl.ds(zrow, zb), :]
    pl.semaphore_wait(bar, len(peers))

    for k in sorted(range(1, nz), key=lambda d: -min(d, nz - d)):
        to = pl.multiple_of(zz(k) * zb, 16)
        send(og_ref.at[pl.ds(to, zb)], zrx.at[pl.ds(zrow, zb)], zs.at[k], zr.at[k], dz=zz(k))
    for k in range(1, nx):
        send(kv_ref, kvb.at[z, x], kxs.at[k], kxr.at[k], dx=xx(k))
    send(q_ref, qb.at[m], qs.at[0], qr.at[0], dc=oc)
    send(q_ref, qb.at[m], qs.at[1], qr.at[1], dy=ysw)
    send(q_ref, qb.at[m], qs.at[2], qr.at[2], dy=ysw, dc=oc)

    lwo.wait()
    for k in (1, 7, 2, 6, 3, 5, 4):
        send(wall.at[x, c, y], wall.at[x, c, y], wys.at[k], wyr.at[k], dy=yy(k))

    for j in range(8):
        qd[j] = jnp.zeros((128, 512), BF)
        acc[j] = jnp.zeros((ODIM, 256), F32)

    def ring(step, i):
        if step < nz // 2:
            g = kvb.at[zz(-step), xx(i)]
            send(g, g, rrs.at[step, i], rrr.at[step, i], dz=zz(1))
        if step < (nz - 1) // 2:
            g = kvb.at[zz(step), xx(i)]
            send(g, g, rls.at[step, i], rlr.at[step, i], dz=zz(-1))

    def ring_wait(step):
        got = []
        if step < nz // 2:
            got.append(zz(-step - 1))
        if step < (nz - 1) // 2:
            got.append(zz(step + 1))
        for i in range(nx):
            if step < nz // 2:
                g = kvb.at[zz(-step - 1), xx(i)]
                rc(g, g, rrs.at[step, i], rrr.at[step, i]).wait_recv()
            if step < (nz - 1) // 2:
                g = kvb.at[zz(step + 1), xx(i)]
                rc(g, g, rls.at[step, i], rlr.at[step, i]).wait_recv()
            ring(step + 1, i)
        return got

    for k in range(1, nz):
        frm = pl.multiple_of(zz(-k) * zb, 16)
        rc(og_ref.at[pl.ds(0, zb)], zrx.at[pl.ds(frm, zb)], zs.at[k], zr.at[k]).wait_recv()
    xsb[...] = dot_t(pb_ref[...], zrx[...]).astype(BF)
    cl = pl.multiple_of(c * 128, 128)
    ocl = pl.multiple_of(oc * 128, 128)
    xrow = pl.multiple_of(x * xbk, 16)
    slots = (yy(0), yy(4))
    for i in range(2):
        xb[slots[i], pl.ds(xrow, xbk), pl.ds(cl, 128)] = xsb[pl.ds(xrow, xbk), i * 128 : (i + 1) * 128]
    for k in sorted(range(1, nx), key=lambda d: -min(d, nx - d)):
        to = pl.multiple_of(xx(k) * xbk, 16)
        for i in range(2):
            send(
                xsb.at[pl.ds(to, xbk), pl.ds(i * 128, 128)],
                xb.at[slots[i], pl.ds(xrow, xbk), pl.ds(cl, 128)],
                xs.at[i, k], xr.at[i, k], dx=xx(k),
            )

    ring(0, 0)
    for k in range(1, nx):
        rc(kv_ref, kvb.at[z, xx(-k)], kxs.at[k], kxr.at[k]).wait_recv()
        ring(0, nx - k)

    rc(q_ref, qb.at[b * 2 + oc], qs.at[0], qr.at[0]).wait_recv()
    rc(q_ref, qb.at[(1 - b) * 2 + c], qs.at[1], qr.at[1]).wait_recv()
    rc(q_ref, qb.at[(1 - b) * 2 + oc], qs.at[2], qr.at[2]).wait_recv()
    for mt in range(4):
        for rp in range(2):
            pair = [qb[2 * rp + i, :, mt * 128 : (mt + 1) * 128] for i in range(2)]
            pair = jnp.concatenate(pair, axis=1)
            qd[mt * 2 + rp, 0:64, 0:256] = pair
            qd[mt * 2 + rp, 64:128, 256:512] = pair

    def attend(zi):
        keys = kvb[zi, :, 0:64, :].reshape(nx * 64, 128)
        vals = [kvb[zi, i, 64:128, :] for i in range(nx)]
        vals = jnp.concatenate(vals, axis=1)
        vals = jnp.concatenate([vals, jnp.ones((ODIM - 64, nx * 128), BF)], axis=0)

        def project(p):
            parts = []
            for i in range(nx):
                parts.append(p[i * 64 : (i + 1) * 64, 0:256])
                parts.append(p[i * 64 : (i + 1) * 64, 256:512])
            return jnp.concatenate(parts, axis=0)

        scores = [dot(keys, qd[0]), dot(keys, qd[1])]
        held = None
        for j in range(8):
            p = project(jnp.exp(scores[j]).astype(BF))
            if j < 6:
                scores.append(dot(keys, qd[j + 2]))
            if held is not None:
                acc[j - 1] += dot(vals, held)
            held = p
        acc[7] += dot(vals, held)

    attend(z)

    for k in range(1, nx):
        frm = pl.multiple_of(xx(-k) * xbk, 16)
        for i in range(2):
            rc(
                xsb.at[pl.ds(0, xbk), pl.ds(i * 128, 128)],
                xb.at[slots[i], pl.ds(frm, xbk), pl.ds(cl, 128)],
                xs.at[i, k], xr.at[i, k],
            ).wait_recv()

    def half(slot, which):
        return xb.at[slot, :, pl.ds(which, 128)]

    plan = ((1, 0), (1, 4), (-1, 0), (-1, 4), (2, 0), (-2, 0))
    for i, (k, r) in enumerate(plan):
        g = half(yy(r), cl)
        send(g, g, ys.at[i], yr.at[i], dy=yy(k))

    def swap(r):
        g = half(yy(r), cl)
        send(g, g, ds.at[r], dr.at[r], dc=oc)

    swap(0)
    swap(4)
    for k in range(1, NY):
        g = wall.at[x, c, yy(-k)]
        rc(g, g, wys.at[k], wyr.at[k]).wait_recv()
    for k in range(1, nx):
        send(wall.at[x, c], wall.at[x, c], wxs.at[k], wxr.at[k], dx=xx(k))
    send(wall.at[x, c], wall.at[x, c], wds.at[0], wdr.at[0], dc=oc)

    def arrive(i):
        k, r = plan[i]
        g = half(yy(r - k), cl)
        rc(g, g, ys.at[i], yr.at[i]).wait_recv()
        swap((r - k + NY) % NY)

    steps = max(nz // 2, (nz - 1) // 2)
    for step in range(max(steps - 2, 0)):
        for zi in ring_wait(step):
            attend(zi)
    def first_layer(r, fresh):
        s = yy(r)
        g = half(s, ocl)
        rc(g, g, ds.at[r], dr.at[r]).wait_recv()
        w0 = pl.multiple_of(s * 256, 256)
        gd = dot(xb[s], wg[pl.ds(w0, 256), :])
        ud = dot(xb[s], wu[pl.ds(w0, 256), :])
        if fresh:
            ga[...] = gd
            up[...] = ud
        else:
            ga[...] += gd
            up[...] += ud

    lwg.wait()
    lwu.wait()
    first_layer(0, True)
    first_layer(4, False)
    coming = (0, 2, 1, 3, 4, 5)
    for n, i in enumerate(coming):
        arrive(i)
        if n >= 1:
            k, r = plan[coming[n - 1]]
            first_layer((r - k + NY) % NY, False)
    later = ring_wait(steps - 2) if steps > 1 else []
    k, r = plan[coming[5]]
    first_layer((r - k + NY) % NY, False)
    gate = ga[...]
    hid = (gate / (1.0 + jnp.exp(-gate)) * up[...]).astype(BF)
    for copy in lwd:
        copy.wait()
    def paired(r):
        rc(pbuf.at[r], prx.at[r], es.at[r], er.at[r]).wait_recv()
        return own[r] + prx[r].astype(F32)

    order = (4, 3, 5, 1, 7, 2, 6, 0)
    route = {4: (0, yy(0 - 2 * sgn)), 3: (1, yy(1)), 5: (2, yy(-1)), 1: (3, yy(1)), 7: (4, yy(-1))}
    for n in range(8 + 2):
        if n < 8:
            r = order[n]
            tmp[r % 2] = dot(hid, wd[yy(r)])
            own[r] = tmp[r % 2, :, pl.ds(cl, 128)]
            pbuf[r] = tmp[r % 2, :, pl.ds(ocl, 128)].astype(BF)
            send(pbuf.at[r], prx.at[r], es.at[r], er.at[r], dc=oc)
        if n >= 2 and order[n - 2] in route:
            r = order[n - 2]
            i, dest = route[r]
            psb[r] = paired(r).astype(BF)
            send(psb.at[r], rs.at[i], ms.at[i], mr.at[i], dy=dest)

    def got_rs(i):
        rc(psb.at[0], rs.at[i], ms.at[i], mr.at[i]).wait_recv()
        return rs[i].astype(F32)

    for zi in later:
        attend(zi)
    far_sum = got_rs(0)
    right = c.astype(F32)
    psb[2] = (paired(2) + got_rs(1) + far_sum * right).astype(BF)
    send(psb.at[2], rs.at[5], ms.at[5], mr.at[5], dy=yy(2))
    psb[6] = (paired(6) + got_rs(2) + far_sum * (1.0 - right)).astype(BF)
    send(psb.at[6], rs.at[6], ms.at[6], mr.at[6], dy=yy(-2))

    for zi in ring_wait(steps - 1):
        attend(zi)
    for j in range(8):
        a = acc[j]
        den = a[64:ODIM]
        hi = den.astype(BF)
        lo = (den - hi.astype(F32)).astype(BF)
        first = lax.broadcasted_iota(jnp.int32, (ODIM - 64, 256), 0) == 0
        ob[j, 0:64] = a[0:64].astype(BF)
        ob[j, 64:ODIM] = jnp.where(first, hi.astype(F32), lo.astype(F32)).astype(BF)
    members = ((0, y, oc, b * 2 + oc), (1, ysw, c, (1 - b) * 2 + c), (2, ysw, oc, (1 - b) * 2 + oc))
    for i, dy, dc, mm in members:
        send(ob.at[pl.ds(2 * mm, 2)], orx.at[i], ts.at[i], tr.at[i], dy=dy, dc=dc)

    ret[...] = (paired(0) + got_rs(3) + got_rs(4) + got_rs(5) + got_rs(6)).astype(BF)
    rbk[pl.ds(xrow, xbk), :] = ret[pl.ds(xrow, xbk), :]
    for k in sorted(range(1, nx), key=lambda d: -min(d, nx - d)):
        to = pl.multiple_of(xx(k) * xbk, 16)
        send(ret.at[pl.ds(to, xbk)], rbk.at[pl.ds(xrow, xbk)], vs.at[k], vr.at[k], dx=xx(k))
    for k in range(1, nx):
        g = wall.at[xx(-k), c]
        rc(g, g, wxs.at[k], wxr.at[k]).wait_recv()
        send(g, g, wds.at[k], wdr.at[k], dc=oc)
    for i, dy, dc, mm in members:
        rc(ob.at[pl.ds(0, 2)], orx.at[i], ts.at[i], tr.at[i]).wait_recv()
    heads = []
    for rp in range(2):
        t = ob[2 * m + rp].astype(F32)
        for i in range(3):
            t += orx[i, rp].astype(F32)
        o = (t[0:64] / (t[64:65] + t[65:66])).astype(BF)
        heads += [o[:, 0:128], o[:, 128:256]]
    heads = jnp.concatenate(heads, axis=0)
    square = (iota((256, 256), 0) == iota((256, 256), 1)).astype(F32).astype(BF)
    ho[...] = dot_t(heads, square).astype(BF).reshape(4, 32, 256)
    hb[h] = ho[h]
    for k in range(1, 4):
        send(ho.at[lax.rem(h + k, 4)], hb.at[h], as_.at[k - 1], ar.at[k - 1], dy=yy(2 * k))

    for k in range(1, nx):
        frm = pl.multiple_of(xx(-k) * xbk, 16)
        rc(ret.at[pl.ds(0, xbk)], rbk.at[pl.ds(frm, xbk)], vs.at[k], vr.at[k]).wait_recv()
    t2[...] = dot(pb_ref[...], rbk[...]).astype(BF)
    fin[pl.ds(zrow, zb), :] = t2[pl.ds(zrow, zb), :]
    for k in sorted(range(1, nz), key=lambda d: -min(d, nz - d)):
        to = pl.multiple_of(zz(k) * zb, 16)
        send(t2.at[pl.ds(to, zb)], fin.at[pl.ds(zrow, zb)], us.at[k], ur.at[k], dz=zz(k))

    for k in range(1, nx):
        g = wall.at[xx(-k), oc]
        rc(g, g, wds.at[k], wdr.at[k]).wait_recv()
    rc(wall.at[x, oc], wall.at[x, oc], wds.at[0], wdr.at[0]).wait_recv()
    for k in range(1, 4):
        rc(ho.at[0], hb.at[lax.rem(h - k + 4, 4)], as_.at[k - 1], ar.at[k - 1]).wait_recv()
    columns = []
    for n in range(nx):
        part = None
        for g in range(4):
            w = jnp.concatenate([wall[n, r % 2, 2 * g + r // 2] for r in range(4)], axis=0)
            part = dot(hb[g], w) if part is None else part + dot(hb[g], w)
        columns.append(part)
    mixed = jnp.concatenate(columns, axis=1)
    scale = lax.rsqrt(jnp.mean(mixed * mixed, axis=1, keepdims=True) + EPSILON)
    lpost.wait()
    out_ref[...] = (mixed * scale * pg_ref[...]).astype(BF)

    logits = lg_ref[...]
    grown = jnp.exp(logits - jnp.max(logits, axis=0, keepdims=True))
    weight = lax.dot_general(
        eye, grown / jnp.sum(grown, axis=0, keepdims=True), (((1,), (1,)), ((), ())),
        precision=lax.Precision.HIGHEST, preferred_element_type=F32,
    )

    for k in range(1, nz):
        frm = pl.multiple_of(zz(-k) * zb, 16)
        rc(t2.at[pl.ds(0, zb)], fin.at[pl.ds(frm, zb)], us.at[k], ur.at[k]).wait_recv()
    total = weight[:, 0:1] * dot(pick[0].astype(F32).astype(BF), fin[...])
    total += weight[:, 1:2] * dot(pick[1].astype(F32).astype(BF), fin[...])
    moe_ref[...] = total.astype(BF)
    for copy in sent:
        copy.wait_send()


def call(nz, nx, cap, *args):
    rows = nz * nx * cap
    vm = pl.BlockSpec(memory_space=pltpu.VMEM)
    hbm = pl.BlockSpec(memory_space=pltpu.HBM)
    dma = lambda *n: pltpu.SemaphoreType.DMA(n)
    big = lambda *s: pltpu.VMEM(s, BF)
    wide = lambda *s: pltpu.VMEM(s, F32)
    scratch = [
        big(64, 512), big(128, 128), big(128, 128), big(128, 2048), wide(1, 2048), wide(1, 2048),
        big(64, 512), big(128, 128), big(rows, 256), big(rows, rows),
        big(nz, nx, 128, 128), big(4, 64, 512), big(8, 128, 512), wide(8, ODIM, 256), big(8, ODIM, 256),
        big(3, 2, ODIM, 256), big(nx, 2, NY, 64, 2048 // nx), big(4, 32, 256), big(4, 32, 256),
        big(rows, 256), big(rows, 256), big(NY, rows, 256), big(2048, 256), big(2048, 256), big(NY, 256, 256),
        wide(rows, 256), wide(rows, 256), wide(2, rows, 256), wide(NY, rows, 128), big(NY, rows, 128),
        big(NY, rows, 128), big(NY, rows, 128), big(7, rows, 128), big(rows, 128), big(rows, 128),
        big(rows, 128), big(rows, 128),
        dma(17), dma(nx), dma(nx), dma(nz, nx), dma(nz, nx), dma(nz, nx), dma(nz, nx), dma(3), dma(3), dma(3), dma(3), dma(NY), dma(NY), dma(nx), dma(nx),
        dma(nx), dma(nx), dma(3), dma(3),
        dma(nz), dma(nz), dma(2, nx), dma(2, nx), dma(6), dma(6), dma(8), dma(8), dma(8), dma(8), dma(7), dma(7),
        dma(nx), dma(nx), dma(nz), dma(nz),
    ]
    return pl.pallas_call(
        functools.partial(kernel, nz, nx, cap),
        out_shape=(jax.ShapeDtypeStruct((32, 2048), BF), jax.ShapeDtypeStruct((128, 128), BF)),
        in_specs=[vm] * 6 + [hbm] * 10,
        out_specs=(vm, vm),
        scratch_shapes=scratch,
        compiler_params=pltpu.CompilerParams(
            collective_id=0, has_side_effects=True, vmem_limit_bytes=67043328 - 200 * 1024
        ),
        name="layer",
    )(*args)


def per_device(
    q_in, k_in, v_in, q_gain, k_gain, w_out, post_gain, moe_in, routes, route_logits, pre_gain, w_gate, w_up, w_down
):
    nz, nx = lax.axis_size("z"), lax.axis_size("x")
    count, top = routes.shape
    experts = nz * nx
    cap = max(2, 3 * top * count // (2 * experts))
    i = np.arange(experts * cap, dtype=np.int32)
    src = (i % (nz * cap)) // cap * (nx * cap) + i // (nz * cap) * cap + i % cap
    return call(
        nz, nx, cap, jnp.asarray(angle_table()), q_gain[None, :], k_gain[None, :], routes.T, route_logits.T,
        jnp.asarray(src[None, :]), pre_gain[None, :], post_gain[None, :],
        q_in.T, k_in, v_in, moe_in, w_gate[0], w_up[0], w_down[0], w_out,
    )


def solution(mesh):
    ny = mesh.shape["tp"] // 2
    nz = 8 if mesh.shape["ep"] % 8 == 0 else 2
    finer = Mesh(mesh.devices.reshape(nz, mesh.shape["ep"] // nz, ny, 2), ALL)
    in_specs = (
        P(EP, TP), P(EP, None), P(EP, None), P(), P(), P(TP, None), P(), P(EP, None), P(EP, None), P(EP, None), P(),
        P(EP, None, TP), P(EP, None, TP), P(EP, TP, None),
    )
    return jax.shard_map(
        per_device, mesh=finer, in_specs=in_specs, out_specs=(P(ALL, None), P(EP, TP)), check_vma=False
    )
```

```python
import functools

import jax
import jax.numpy as jnp
import numpy as np
from jax import lax
from jax.experimental import pallas as pl
from jax.experimental.pallas import tpu as pltpu
from jax.sharding import Mesh
from jax.sharding import PartitionSpec as P

GRID_W = 128
EPSILON = 1e-06
ROPE_BASE = 10000.0
EP = ("z", "x")
TP = ("y", "c")
ALL = ("z", "x", "y", "c")
NY = 8
ODIM = 80
MESH = pl.DeviceIdType.MESH
BF = jnp.bfloat16
F32 = jnp.float32


def angle_table():
    lane = np.arange(128)
    inverse = np.float32(ROPE_BASE) ** (-np.arange(16, dtype=np.float32) / np.float32(16))
    angle = (np.arange(GRID_W, dtype=np.float32)[:, None] * inverse[None, lane % 16]).astype(np.float64)
    sign = np.where(lane % 32 < 16, -1.0, 1.0)[None, :]
    return np.where(lane[None, :] < 64, np.cos(angle), sign * np.sin(angle)).astype(np.float32)


def dot(a, b):
    return jnp.dot(a, b, preferred_element_type=F32)


def dot_t(a, b):
    return lax.dot_general(a, b, (((0,), (0,)), ((), ())), preferred_element_type=F32)


def dot_nt(a, b):
    return lax.dot_general(a, b, (((1,), (1,)), ((), ())), preferred_element_type=F32)


def iota(shape, dim):
    return lax.broadcasted_iota(jnp.int32, shape, dim)


def kernel(
    nz, nx, cap,
    tab_ref, qg_ref, kg_ref, rt_ref, lg_ref, src_ref, pre_hbm, post_hbm, q_hbm, k_hbm, v_hbm, x_hbm, wg_hbm, wu_hbm, wd_hbm, wo_hbm,
    out_ref, moe_ref,
    qv, kv, vv, xv, prev, pg_ref, q_ref, kv_ref, og_ref, pb_ref,
    kvb, qb, qd, acc, ob, orx, wall, ho, hb,
    zrx, xsb, xb, wg, wu, wd, ga, up, tmp, own, pbuf, prx, psb, rs, ret, rbk, t2, fin,
    lsem, kxs, kxr, rrs, rrr, rls, rlr, qs, qr, ts, tr, wys, wyr, wxs, wxr, wds, wdr, as_, ar,
    zs, zr, xs, xr, ys, yr, ds, dr, es, er, ms, mr, vs, vr, us, ur,
):
    z, x, y, c = (lax.axis_index(n) for n in ALL)
    rows = nz * nx * cap
    zb, xbk = nx * cap, nz * cap
    b = lax.rem(y, 2)
    h = y // 2
    m = b * 2 + c
    ysw = y + 1 - 2 * b
    oc = 1 - c
    sgn = 1 - 2 * c

    def yy(k):
        return lax.rem(y + (k + 2 * NY), NY)

    def zz(k):
        return lax.rem(z + (k + nz), nz)

    def xx(k):
        return lax.rem(x + (k + nx), nx)

    sent = []

    def rc(src, dst, ss, rr, dz=None, dx=None, dy=None, dc=None):
        dev = (z if dz is None else dz, x if dx is None else dx, y if dy is None else dy, c if dc is None else dc)
        return pltpu.make_async_remote_copy(src, dst, ss, rr, device_id=dev, device_id_type=MESH)

    def send(*args, **kw):
        copy = rc(*args, **kw)
        copy.start()
        sent.append(copy)

    def local(src, dst, i):
        copy = pltpu.make_async_copy(src, dst, lsem.at[i])
        copy.start()
        return copy

    ep = z * nx + x
    hl = pl.multiple_of((h // 2) * 128, 128)
    mrow = pl.multiple_of(m * 128, 128)
    lk = local(k_hbm.at[pl.ds(mrow, 128), pl.ds(hl, 128)], kv, 11)
    lv = local(v_hbm.at[pl.ds(mrow, 128), pl.ds(hl, 128)], vv, 12)
    lx = local(x_hbm, xv, 13)
    lq = local(q_hbm, qv, 14)
    lpre = local(pre_hbm, prev, 15)
    lpost = local(post_hbm, pg_ref, 16)
    wc = 2048 // nx
    lwo = local(wo_hbm.at[:, pl.ds(pl.multiple_of(x * wc, 128), wc)], wall.at[x, c, y], 0)
    lwg = local(wg_hbm, wg, 1)
    lwu = local(wu_hbm, wu, 2)
    lwd = [local(wd_hbm.at[:, k * 256 : (k + 1) * 256], wd.at[k], 3 + k) for k in range(NY)]

    bar = pltpu.get_barrier_semaphore()
    peers = [(zz(k), x, y, c) for k in range(1, nz)]
    peers += [(z, xx(k), y, c) for k in range(1, nx)]
    peers += [(z, x, yy(k), c) for k in (1, -1, 2, -2, 3, -3, 4)]
    peers += [(z, x, y, oc), (z, x, ysw, oc)]
    for peer in peers:
        pl.semaphore_signal(bar, inc=1, device_id=peer, device_id_type=MESH)

    def mixer(j, l):
        i = j - 64
        return ((l < 64) & (i == l)) | ((l >= 64) & (i == ((l - 64) ^ 16)))

    wide_mix = mixer(iota((192, 128), 0), iota((192, 128), 1)).astype(F32).astype(BF)
    sub = lax.rem(h, 2)
    hmix = mixer(iota((128, 128), 0) + (1 - sub) * 64, iota((128, 128), 1)).astype(F32).astype(BF)
    qmix = wide_mix[64:128]
    lane = iota((128, 128), 1)
    row_lane = (lane & 63) < 32
    col_table = tab_ref[...]

    def gains(ref):
        return jnp.dot(
            jnp.broadcast_to(ref[...], (8, 64)), qmix.astype(F32), precision=lax.Precision.HIGHEST,
            preferred_element_type=F32,
        )[0:1]

    def turned(values, gain, r):
        table = jnp.where(row_lane, tab_ref[pl.ds(r, 1), :], col_table) * gain
        scale = lax.rsqrt(jnp.mean(values * values, axis=1, keepdims=True) + EPSILON)
        out = values * scale * table
        return out + pltpu.roll(out, 64, 1)

    kgain = gains(kg_ref)
    lk.wait()
    k128 = turned(dot(kv[...], hmix), kgain, ep * 4 + m)
    kv_ref[0:64] = jnp.where(lane[0:64] < 64, k128[0:64], k128[64:128]).astype(BF)
    lv.wait()
    pick = (iota((64, 128), 1) == iota((64, 128), 0) + 64 * sub).astype(F32).astype(BF)
    kv_ref[64:128] = dot_nt(pick, vv[...]).astype(BF)
    kvb[z, x] = kv_ref[...]

    count = xv.shape[0]
    experts = nz * nx
    lx.wait()
    x32 = xv[...].astype(F32)
    xscale = lax.rsqrt(jnp.mean(x32 * x32, axis=1, keepdims=True) + EPSILON)
    lpre.wait()
    normed = []
    for i in range(2):
        col = pl.multiple_of((yy(4 * i) * 2 + c) * 128, 128)
        normed.append((xv[:, pl.ds(col, 128)].astype(F32) * xscale * prev[:, pl.ds(col, 128)]).astype(BF))
    normed = jnp.concatenate(normed, axis=1)
    eid = iota((count, 128), 1)
    eye = (iota((count, count), 1) == iota((count, count), 0)).astype(F32)
    named = dot_nt(eye.astype(BF), rt_ref[...].astype(F32).astype(BF)).astype(jnp.int32)
    hot = [eid == named[:, i : i + 1] for i in range(2)]
    lower = (iota((count, count), 1) < iota((count, count), 0)).astype(F32).astype(BF)
    rank = dot(lower, (hot[0] | hot[1]).astype(F32).astype(BF)) + (cap * eid).astype(F32)
    place = [jnp.sum(jnp.where(hh, rank, 0.0), axis=1, keepdims=True).astype(jnp.int32) for hh in hot]
    slot = iota((count, rows), 1)
    pick = [slot == pp for pp in place]
    og_ref[...] = dot_t((pick[0] | pick[1]).astype(F32).astype(BF), normed).astype(BF)
    pb_ref[...] = (iota((rows, rows), 0) == src_ref[...]).astype(F32).astype(BF)

    lq.wait()
    q128 = dot_t(qv[...], qmix)
    qgain = gains(qg_ref)
    turned_q = [turned(q128[i * 128 : (i + 1) * 128], qgain, ep * 4 + i).astype(BF) for i in range(4)]
    ordered = [turned_q[i][k * 32 : (k + 1) * 32] for k in range(4) for i in range(4)]
    ordered = jnp.concatenate(ordered, axis=0) * BF(0.125)
    pick_q = (iota((64, 128), 1) == iota((64, 128), 0)).astype(F32).astype(BF)
    q_ref[...] = dot_nt(pick_q, ordered).astype(BF)
    qb[m] = q_ref[...]
    zrow = pl.multiple_of(z * zb, 16)
    zrx[pl.ds(zrow, zb), :] = og_ref[pl.ds(zrow, zb), :]
    pl.semaphore_wait(bar, len(peers))

    for k in sorted(range(1, nz), key=lambda d: -min(d, nz - d)):
        to = pl.multiple_of(zz(k) * zb, 16)
        send(og_ref.at[pl.ds(to, zb)], zrx.at[pl.ds(zrow, zb)], zs.at[k], zr.at[k], dz=zz(k))
    for k in range(1, nx):
        send(kv_ref, kvb.at[z, x], kxs.at[k], kxr.at[k], dx=xx(k))
    send(q_ref, qb.at[m], qs.at[0], qr.at[0], dc=oc)
    send(q_ref, qb.at[m], qs.at[1], qr.at[1], dy=ysw)
    send(q_ref, qb.at[m], qs.at[2], qr.at[2], dy=ysw, dc=oc)

    lwo.wait()
    for k in (1, 7, 2, 6, 3, 5, 4):
        send(wall.at[x, c, y], wall.at[x, c, y], wys.at[k], wyr.at[k], dy=yy(k))

    def spread(k):
        g = wall.at[x, c, yy(-k)]
        if k:
            rc(g, g, wys.at[k], wyr.at[k]).wait_recv()
        for j in range(1, nx):
            send(g, g, wxs.at[k, j], wxr.at[k, j], dx=xx(j))

    spread(0)

    for j in range(8):
        qd[j] = jnp.zeros((128, 512), BF)
        acc[j] = jnp.zeros((ODIM, 256), F32)

    def ring(step, i):
        if step < nz // 2:
            g = kvb.at[zz(-step), xx(i)]
            send(g, g, rrs.at[step, i], rrr.at[step, i], dz=zz(1))
        if step < (nz - 1) // 2:
            g = kvb.at[zz(step), xx(i)]
            send(g, g, rls.at[step, i], rlr.at[step, i], dz=zz(-1))

    def ring_wait(step):
        got = []
        if step < nz // 2:
            got.append(zz(-step - 1))
        if step < (nz - 1) // 2:
            got.append(zz(step + 1))
        for i in range(nx):
            if step < nz // 2:
                g = kvb.at[zz(-step - 1), xx(i)]
                rc(g, g, rrs.at[step, i], rrr.at[step, i]).wait_recv()
            if step < (nz - 1) // 2:
                g = kvb.at[zz(step + 1), xx(i)]
                rc(g, g, rls.at[step, i], rlr.at[step, i]).wait_recv()
            ring(step + 1, i)
        return got

    for k in range(1, nz):
        frm = pl.multiple_of(zz(-k) * zb, 16)
        rc(og_ref.at[pl.ds(0, zb)], zrx.at[pl.ds(frm, zb)], zs.at[k], zr.at[k]).wait_recv()
    xsb[...] = dot_t(pb_ref[...], zrx[...]).astype(BF)
    cl = pl.multiple_of(c * 128, 128)
    ocl = pl.multiple_of(oc * 128, 128)
    xrow = pl.multiple_of(x * xbk, 16)
    slots = (yy(0), yy(4))
    for i in range(2):
        xb[slots[i], pl.ds(xrow, xbk), pl.ds(cl, 128)] = xsb[pl.ds(xrow, xbk), i * 128 : (i + 1) * 128]
    for k in sorted(range(1, nx), key=lambda d: -min(d, nx - d)):
        to = pl.multiple_of(xx(k) * xbk, 16)
        for i in range(2):
            send(
                xsb.at[pl.ds(to, xbk), pl.ds(i * 128, 128)],
                xb.at[slots[i], pl.ds(xrow, xbk), pl.ds(cl, 128)],
                xs.at[i, k], xr.at[i, k], dx=xx(k),
            )

    for k in (1, 7, 2, 6):
        spread(k)
    ring(0, 0)
    for k in range(1, nx):
        rc(kv_ref, kvb.at[z, xx(-k)], kxs.at[k], kxr.at[k]).wait_recv()
        ring(0, nx - k)

    rc(q_ref, qb.at[b * 2 + oc], qs.at[0], qr.at[0]).wait_recv()
    rc(q_ref, qb.at[(1 - b) * 2 + c], qs.at[1], qr.at[1]).wait_recv()
    rc(q_ref, qb.at[(1 - b) * 2 + oc], qs.at[2], qr.at[2]).wait_recv()
    for mt in range(4):
        for rp in range(2):
            pair = [qb[2 * rp + i, :, mt * 128 : (mt + 1) * 128] for i in range(2)]
            pair = jnp.concatenate(pair, axis=1)
            qd[mt * 2 + rp, 0:64, 0:256] = pair
            qd[mt * 2 + rp, 64:128, 256:512] = pair

    def attend(zi):
        keys = kvb[zi, :, 0:64, :].reshape(nx * 64, 128)
        vals = [kvb[zi, i, 64:128, :] for i in range(nx)]
        vals = jnp.concatenate(vals, axis=1)
        vals = jnp.concatenate([vals, jnp.ones((ODIM - 64, nx * 128), BF)], axis=0)

        def project(p):
            parts = []
            for i in range(nx):
                parts.append(p[i * 64 : (i + 1) * 64, 0:256])
                parts.append(p[i * 64 : (i + 1) * 64, 256:512])
            return jnp.concatenate(parts, axis=0)

        scores = [dot(keys, qd[0]), dot(keys, qd[1])]
        held = None
        for j in range(8):
            p = project(jnp.exp(scores[j]).astype(BF))
            if j < 6:
                scores.append(dot(keys, qd[j + 2]))
            if held is not None:
                acc[j - 1] += dot(vals, held)
            held = p
        acc[7] += dot(vals, held)

    attend(z)

    for k in range(1, nx):
        frm = pl.multiple_of(xx(-k) * xbk, 16)
        for i in range(2):
            rc(
                xsb.at[pl.ds(0, xbk), pl.ds(i * 128, 128)],
                xb.at[slots[i], pl.ds(frm, xbk), pl.ds(cl, 128)],
                xs.at[i, k], xr.at[i, k],
            ).wait_recv()

    def half(slot, which):
        return xb.at[slot, :, pl.ds(which, 128)]

    plan = ((1, 0), (1, 4), (-1, 0), (-1, 4), (2, 0), (-2, 0))
    for i, (k, r) in enumerate(plan):
        g = half(yy(r), cl)
        send(g, g, ys.at[i], yr.at[i], dy=yy(k))

    def swap(r):
        g = half(yy(r), cl)
        send(g, g, ds.at[r], dr.at[r], dc=oc)

    swap(0)
    swap(4)
    for k in (3, 5, 4):
        spread(k)
    send(wall.at[x, c], wall.at[x, c], wds.at[0], wdr.at[0], dc=oc)

    def arrive(i):
        k, r = plan[i]
        g = half(yy(r - k), cl)
        rc(g, g, ys.at[i], yr.at[i]).wait_recv()
        swap((r - k + NY) % NY)

    steps = max(nz // 2, (nz - 1) // 2)
    for step in range(max(steps - 2, 0)):
        for zi in ring_wait(step):
            attend(zi)
    def first_layer(r, fresh):
        s = yy(r)
        g = half(s, ocl)
        rc(g, g, ds.at[r], dr.at[r]).wait_recv()
        w0 = pl.multiple_of(s * 256, 256)
        gd = dot(xb[s], wg[pl.ds(w0, 256), :])
        ud = dot(xb[s], wu[pl.ds(w0, 256), :])
        if fresh:
            ga[...] = gd
            up[...] = ud
        else:
            ga[...] += gd
            up[...] += ud

    lwg.wait()
    lwu.wait()
    first_layer(0, True)
    first_layer(4, False)
    coming = (0, 2, 1, 3, 4, 5)
    for n, i in enumerate(coming):
        arrive(i)
        if n >= 1:
            k, r = plan[coming[n - 1]]
            first_layer((r - k + NY) % NY, False)
    later = ring_wait(steps - 2) if steps > 1 else []
    k, r = plan[coming[5]]
    first_layer((r - k + NY) % NY, False)
    gate = ga[...]
    hid = (gate / (1.0 + jnp.exp(-gate)) * up[...]).astype(BF)
    for copy in lwd:
        copy.wait()
    def paired(r):
        rc(pbuf.at[r], prx.at[r], es.at[r], er.at[r]).wait_recv()
        return own[r] + prx[r].astype(F32)

    order = (4, 3, 5, 1, 7, 2, 6, 0)
    route = {4: (0, yy(0 - 2 * sgn)), 3: (1, yy(1)), 5: (2, yy(-1)), 1: (3, yy(1)), 7: (4, yy(-1))}
    for n in range(8 + 2):
        if n < 8:
            r = order[n]
            tmp[r % 2] = dot(hid, wd[yy(r)])
            own[r] = tmp[r % 2, :, pl.ds(cl, 128)]
            pbuf[r] = tmp[r % 2, :, pl.ds(ocl, 128)].astype(BF)
            send(pbuf.at[r], prx.at[r], es.at[r], er.at[r], dc=oc)
        if n >= 2 and order[n - 2] in route:
            r = order[n - 2]
            i, dest = route[r]
            psb[r] = paired(r).astype(BF)
            send(psb.at[r], rs.at[i], ms.at[i], mr.at[i], dy=dest)

    def got_rs(i):
        rc(psb.at[0], rs.at[i], ms.at[i], mr.at[i]).wait_recv()
        return rs[i].astype(F32)

    for zi in later:
        attend(zi)
    far_sum = got_rs(0)
    right = c.astype(F32)
    psb[2] = (paired(2) + got_rs(1) + far_sum * right).astype(BF)
    send(psb.at[2], rs.at[5], ms.at[5], mr.at[5], dy=yy(2))
    psb[6] = (paired(6) + got_rs(2) + far_sum * (1.0 - right)).astype(BF)
    send(psb.at[6], rs.at[6], ms.at[6], mr.at[6], dy=yy(-2))

    for zi in ring_wait(steps - 1):
        attend(zi)
    for j in range(8):
        a = acc[j]
        den = a[64:ODIM]
        hi = den.astype(BF)
        lo = (den - hi.astype(F32)).astype(BF)
        first = lax.broadcasted_iota(jnp.int32, (ODIM - 64, 256), 0) == 0
        ob[j, 0:64] = a[0:64].astype(BF)
        ob[j, 64:ODIM] = jnp.where(first, hi.astype(F32), lo.astype(F32)).astype(BF)
    members = ((0, y, oc, b * 2 + oc), (1, ysw, c, (1 - b) * 2 + c), (2, ysw, oc, (1 - b) * 2 + oc))
    for i, dy, dc, mm in members:
        send(ob.at[pl.ds(2 * mm, 2)], orx.at[i], ts.at[i], tr.at[i], dy=dy, dc=dc)

    ret[...] = (paired(0) + got_rs(3) + got_rs(4) + got_rs(5) + got_rs(6)).astype(BF)
    rbk[pl.ds(xrow, xbk), :] = ret[pl.ds(xrow, xbk), :]
    for k in sorted(range(1, nx), key=lambda d: -min(d, nx - d)):
        to = pl.multiple_of(xx(k) * xbk, 16)
        send(ret.at[pl.ds(to, xbk)], rbk.at[pl.ds(xrow, xbk)], vs.at[k], vr.at[k], dx=xx(k))
    for k in range(1, nx):
        for j in range(NY):
            g = wall.at[xx(-k), c, yy(-j)]
            rc(g, g, wxs.at[j, k], wxr.at[j, k]).wait_recv()
        g = wall.at[xx(-k), c]
        send(g, g, wds.at[k], wdr.at[k], dc=oc)
    for i, dy, dc, mm in members:
        rc(ob.at[pl.ds(0, 2)], orx.at[i], ts.at[i], tr.at[i]).wait_recv()
    heads = []
    for rp in range(2):
        t = ob[2 * m + rp].astype(F32)
        for i in range(3):
            t += orx[i, rp].astype(F32)
        o = (t[0:64] / (t[64:65] + t[65:66])).astype(BF)
        heads += [o[:, 0:128], o[:, 128:256]]
    heads = jnp.concatenate(heads, axis=0)
    square = (iota((256, 256), 0) == iota((256, 256), 1)).astype(F32).astype(BF)
    ho[...] = dot_t(heads, square).astype(BF).reshape(4, 32, 256)
    hb[h] = ho[h]
    for k in range(1, 4):
        send(ho.at[lax.rem(h + k, 4)], hb.at[h], as_.at[k - 1], ar.at[k - 1], dy=yy(2 * k))

    for k in range(1, nx):
        frm = pl.multiple_of(xx(-k) * xbk, 16)
        rc(ret.at[pl.ds(0, xbk)], rbk.at[pl.ds(frm, xbk)], vs.at[k], vr.at[k]).wait_recv()
    t2[...] = dot(pb_ref[...], rbk[...]).astype(BF)
    fin[pl.ds(zrow, zb), :] = t2[pl.ds(zrow, zb), :]
    for k in sorted(range(1, nz), key=lambda d: -min(d, nz - d)):
        to = pl.multiple_of(zz(k) * zb, 16)
        send(t2.at[pl.ds(to, zb)], fin.at[pl.ds(zrow, zb)], us.at[k], ur.at[k], dz=zz(k))

    for k in range(1, nx):
        g = wall.at[xx(-k), oc]
        rc(g, g, wds.at[k], wdr.at[k]).wait_recv()
    rc(wall.at[x, oc], wall.at[x, oc], wds.at[0], wdr.at[0]).wait_recv()
    for k in range(1, 4):
        rc(ho.at[0], hb.at[lax.rem(h - k + 4, 4)], as_.at[k - 1], ar.at[k - 1]).wait_recv()
    columns = []
    for n in range(nx):
        part = None
        for g in range(4):
            w = jnp.concatenate([wall[n, r % 2, 2 * g + r // 2] for r in range(4)], axis=0)
            part = dot(hb[g], w) if part is None else part + dot(hb[g], w)
        columns.append(part)
    mixed = jnp.concatenate(columns, axis=1)
    scale = lax.rsqrt(jnp.mean(mixed * mixed, axis=1, keepdims=True) + EPSILON)
    lpost.wait()
    out_ref[...] = (mixed * scale * pg_ref[...]).astype(BF)

    logits = lg_ref[...]
    grown = jnp.exp(logits - jnp.max(logits, axis=0, keepdims=True))
    weight = lax.dot_general(
        eye, grown / jnp.sum(grown, axis=0, keepdims=True), (((1,), (1,)), ((), ())),
        precision=lax.Precision.HIGHEST, preferred_element_type=F32,
    )

    for k in range(1, nz):
        frm = pl.multiple_of(zz(-k) * zb, 16)
        rc(t2.at[pl.ds(0, zb)], fin.at[pl.ds(frm, zb)], us.at[k], ur.at[k]).wait_recv()
    total = weight[:, 0:1] * dot(pick[0].astype(F32).astype(BF), fin[...])
    total += weight[:, 1:2] * dot(pick[1].astype(F32).astype(BF), fin[...])
    moe_ref[...] = total.astype(BF)
    for copy in sent:
        copy.wait_send()


def call(nz, nx, cap, *args):
    rows = nz * nx * cap
    vm = pl.BlockSpec(memory_space=pltpu.VMEM)
    hbm = pl.BlockSpec(memory_space=pltpu.HBM)
    dma = lambda *n: pltpu.SemaphoreType.DMA(n)
    big = lambda *s: pltpu.VMEM(s, BF)
    wide = lambda *s: pltpu.VMEM(s, F32)
    scratch = [
        big(64, 512), big(128, 128), big(128, 128), big(128, 2048), wide(1, 2048), wide(1, 2048),
        big(64, 512), big(128, 128), big(rows, 256), big(rows, rows),
        big(nz, nx, 128, 128), big(4, 64, 512), big(8, 128, 512), wide(8, ODIM, 256), big(8, ODIM, 256),
        big(3, 2, ODIM, 256), big(nx, 2, NY, 64, 2048 // nx), big(4, 32, 256), big(4, 32, 256),
        big(rows, 256), big(rows, 256), big(NY, rows, 256), big(2048, 256), big(2048, 256), big(NY, 256, 256),
        wide(rows, 256), wide(rows, 256), wide(2, rows, 256), wide(NY, rows, 128), big(NY, rows, 128),
        big(NY, rows, 128), big(NY, rows, 128), big(7, rows, 128), big(rows, 128), big(rows, 128),
        big(rows, 128), big(rows, 128),
        dma(17), dma(nx), dma(nx), dma(nz, nx), dma(nz, nx), dma(nz, nx), dma(nz, nx), dma(3), dma(3), dma(3), dma(3), dma(NY), dma(NY), dma(NY, nx), dma(NY, nx),
        dma(nx), dma(nx), dma(3), dma(3),
        dma(nz), dma(nz), dma(2, nx), dma(2, nx), dma(6), dma(6), dma(8), dma(8), dma(8), dma(8), dma(7), dma(7),
        dma(nx), dma(nx), dma(nz), dma(nz),
    ]
    return pl.pallas_call(
        functools.partial(kernel, nz, nx, cap),
        out_shape=(jax.ShapeDtypeStruct((32, 2048), BF), jax.ShapeDtypeStruct((128, 128), BF)),
        in_specs=[vm] * 6 + [hbm] * 10,
        out_specs=(vm, vm),
        scratch_shapes=scratch,
        compiler_params=pltpu.CompilerParams(
            collective_id=0, has_side_effects=True, vmem_limit_bytes=67043328 - 200 * 1024
        ),
        name="layer",
    )(*args)


def per_device(
    q_in, k_in, v_in, q_gain, k_gain, w_out, post_gain, moe_in, routes, route_logits, pre_gain, w_gate, w_up, w_down
):
    nz, nx = lax.axis_size("z"), lax.axis_size("x")
    count, top = routes.shape
    experts = nz * nx
    cap = max(2, 3 * top * count // (2 * experts))
    i = np.arange(experts * cap, dtype=np.int32)
    src = (i % (nz * cap)) // cap * (nx * cap) + i // (nz * cap) * cap + i % cap
    return call(
        nz, nx, cap, jnp.asarray(angle_table()), q_gain[None, :], k_gain[None, :], routes.T, route_logits.T,
        jnp.asarray(src[None, :]), pre_gain[None, :], post_gain[None, :],
        q_in.T, k_in, v_in, moe_in, w_gate[0], w_up[0], w_down[0], w_out,
    )


def solution(mesh):
    ny = mesh.shape["tp"] // 2
    nz = 8 if mesh.shape["ep"] % 8 == 0 else 2
    finer = Mesh(mesh.devices.reshape(nz, mesh.shape["ep"] // nz, ny, 2), ALL)
    in_specs = (
        P(EP, TP), P(EP, None), P(EP, None), P(), P(), P(TP, None), P(), P(EP, None), P(EP, None), P(EP, None), P(),
        P(EP, None, TP), P(EP, None, TP), P(EP, TP, None),
    )
    return jax.shard_map(
        per_device, mesh=finer, in_specs=in_specs, out_specs=(P(ALL, None), P(EP, TP)), check_vma=False
    )
```

```python
import functools

import jax
import jax.numpy as jnp
import numpy as np
from jax import lax
from jax.experimental import pallas as pl
from jax.experimental.pallas import tpu as pltpu
from jax.sharding import Mesh
from jax.sharding import PartitionSpec as P

GRID_W = 128
EPSILON = 1e-06
ROPE_BASE = 10000.0
EP = ("z", "x")
TP = ("y", "c")
ALL = ("z", "x", "y", "c")
NY = 8
ODIM = 80
MESH = pl.DeviceIdType.MESH
BF = jnp.bfloat16
F32 = jnp.float32


def angle_table():
    lane = np.arange(128)
    inverse = np.float32(ROPE_BASE) ** (-np.arange(16, dtype=np.float32) / np.float32(16))
    angle = (np.arange(GRID_W, dtype=np.float32)[:, None] * inverse[None, lane % 16]).astype(np.float64)
    sign = np.where(lane % 32 < 16, -1.0, 1.0)[None, :]
    return np.where(lane[None, :] < 64, np.cos(angle), sign * np.sin(angle)).astype(np.float32)


def dot(a, b):
    return jnp.dot(a, b, preferred_element_type=F32)


def dot_t(a, b):
    return lax.dot_general(a, b, (((0,), (0,)), ((), ())), preferred_element_type=F32)


def dot_nt(a, b):
    return lax.dot_general(a, b, (((1,), (1,)), ((), ())), preferred_element_type=F32)


def iota(shape, dim):
    return lax.broadcasted_iota(jnp.int32, shape, dim)


def kernel(
    nz, nx, cap,
    tab_ref, qg_ref, kg_ref, rt_ref, lg_ref, src_ref, pre_hbm, post_hbm, q_hbm, k_hbm, v_hbm, x_hbm, wg_hbm, wu_hbm, wd_hbm, wo_hbm,
    out_ref, moe_ref,
    qv, kv, vv, xv, prev, pg_ref, q_ref, kv_ref, og_ref, pb_ref,
    kvb, qb, qd, acc, ob, orx, wall, ho, hb,
    zrx, xsb, xb, wg, wu, wd, ga, up, tmp, own, pbuf, prx, psb, rs, ret, rbk, t2, fin,
    lsem, kxs, kxr, rrs, rrr, rls, rlr, qs, qr, ts, tr, wys, wyr, wxs, wxr, wds, wdr, as_, ar,
    zs, zr, xs, xr, ys, yr, ds, dr, es, er, ms, mr, vs, vr, us, ur,
):
    z, x, y, c = (lax.axis_index(n) for n in ALL)
    rows = nz * nx * cap
    zb, xbk = nx * cap, nz * cap
    b = lax.rem(y, 2)
    h = y // 2
    m = b * 2 + c
    ysw = y + 1 - 2 * b
    oc = 1 - c
    sgn = 1 - 2 * c

    def yy(k):
        return lax.rem(y + (k + 2 * NY), NY)

    def zz(k):
        return lax.rem(z + (k + nz), nz)

    def xx(k):
        return lax.rem(x + (k + nx), nx)

    sent = []

    def rc(src, dst, ss, rr, dz=None, dx=None, dy=None, dc=None):
        dev = (z if dz is None else dz, x if dx is None else dx, y if dy is None else dy, c if dc is None else dc)
        return pltpu.make_async_remote_copy(src, dst, ss, rr, device_id=dev, device_id_type=MESH)

    def send(*args, **kw):
        copy = rc(*args, **kw)
        copy.start()
        sent.append(copy)

    def local(src, dst, i):
        copy = pltpu.make_async_copy(src, dst, lsem.at[i])
        copy.start()
        return copy

    ep = z * nx + x
    hl = pl.multiple_of((h // 2) * 128, 128)
    mrow = pl.multiple_of(m * 128, 128)
    lk = local(k_hbm.at[pl.ds(mrow, 128), pl.ds(hl, 128)], kv, 11)
    lv = local(v_hbm.at[pl.ds(mrow, 128), pl.ds(hl, 128)], vv, 12)
    lx = local(x_hbm, xv, 13)
    lq = local(q_hbm, qv, 14)
    lpre = local(pre_hbm, prev, 15)
    lpost = local(post_hbm, pg_ref, 16)
    wc = 2048 // nx
    lwo = local(wo_hbm.at[:, pl.ds(pl.multiple_of(x * wc, 128), wc)], wall.at[x, c, y], 0)
    lwg = local(wg_hbm, wg, 1)
    lwu = local(wu_hbm, wu, 2)
    lwd = [local(wd_hbm.at[:, k * 256 : (k + 1) * 256], wd.at[k], 3 + k) for k in range(NY)]

    bar = pltpu.get_barrier_semaphore()
    peers = [(zz(k), x, y, c) for k in range(1, nz)]
    peers += [(z, xx(k), y, c) for k in range(1, nx)]
    peers += [(z, x, yy(k), c) for k in (1, -1, 2, -2, 3, -3, 4)]
    peers += [(z, x, y, oc), (z, x, ysw, oc)]
    for peer in peers:
        pl.semaphore_signal(bar, inc=1, device_id=peer, device_id_type=MESH)

    def mixer(j, l):
        i = j - 64
        return ((l < 64) & (i == l)) | ((l >= 64) & (i == ((l - 64) ^ 16)))

    wide_mix = mixer(iota((192, 128), 0), iota((192, 128), 1)).astype(F32).astype(BF)
    sub = lax.rem(h, 2)
    hmix = mixer(iota((128, 128), 0) + (1 - sub) * 64, iota((128, 128), 1)).astype(F32).astype(BF)
    qmix = wide_mix[64:128]
    lane = iota((128, 128), 1)
    row_lane = (lane & 63) < 32
    col_table = tab_ref[...]

    def gains(ref):
        return jnp.dot(
            jnp.broadcast_to(ref[...], (8, 64)), qmix.astype(F32), precision=lax.Precision.HIGHEST,
            preferred_element_type=F32,
        )[0:1]

    def turned(values, gain, r):
        table = jnp.where(row_lane, tab_ref[pl.ds(r, 1), :], col_table) * gain
        scale = lax.rsqrt(jnp.mean(values * values, axis=1, keepdims=True) + EPSILON)
        out = values * scale * table
        return out + pltpu.roll(out, 64, 1)

    kgain = gains(kg_ref)
    lk.wait()
    k128 = turned(dot(kv[...], hmix), kgain, ep * 4 + m)
    kv_ref[0:64] = jnp.where(lane[0:64] < 64, k128[0:64], k128[64:128]).astype(BF)
    lv.wait()
    pick = (iota((64, 128), 1) == iota((64, 128), 0) + 64 * sub).astype(F32).astype(BF)
    kv_ref[64:128] = dot_nt(pick, vv[...]).astype(BF)
    kvb[z, x] = kv_ref[...]

    count = xv.shape[0]
    experts = nz * nx
    lx.wait()
    x32 = xv[...].astype(F32)
    xscale = lax.rsqrt(jnp.mean(x32 * x32, axis=1, keepdims=True) + EPSILON)
    lpre.wait()
    normed = []
    for i in range(2):
        col = pl.multiple_of((yy(4 * i) * 2 + c) * 128, 128)
        normed.append((xv[:, pl.ds(col, 128)].astype(F32) * xscale * prev[:, pl.ds(col, 128)]).astype(BF))
    normed = jnp.concatenate(normed, axis=1)
    eid = iota((count, 128), 1)
    eye = (iota((count, count), 1) == iota((count, count), 0)).astype(F32)
    named = dot_nt(eye.astype(BF), rt_ref[...].astype(F32).astype(BF)).astype(jnp.int32)
    hot = [eid == named[:, i : i + 1] for i in range(2)]
    lower = (iota((count, count), 1) < iota((count, count), 0)).astype(F32).astype(BF)
    rank = dot(lower, (hot[0] | hot[1]).astype(F32).astype(BF)) + (cap * eid).astype(F32)
    place = [jnp.sum(jnp.where(hh, rank, 0.0), axis=1, keepdims=True).astype(jnp.int32) for hh in hot]
    slot = iota((count, rows), 1)
    pick = [slot == pp for pp in place]
    og_ref[...] = dot_t((pick[0] | pick[1]).astype(F32).astype(BF), normed).astype(BF)
    pb_ref[...] = (iota((rows, rows), 0) == src_ref[...]).astype(F32).astype(BF)

    lq.wait()
    q128 = dot_t(qv[...], qmix)
    qgain = gains(qg_ref)
    turned_q = [turned(q128[i * 128 : (i + 1) * 128], qgain, ep * 4 + i).astype(BF) for i in range(4)]
    ordered = [turned_q[i][k * 32 : (k + 1) * 32] for k in range(4) for i in range(4)]
    ordered = jnp.concatenate(ordered, axis=0) * BF(0.125)
    pick_q = (iota((64, 128), 1) == iota((64, 128), 0)).astype(F32).astype(BF)
    q_ref[...] = dot_nt(pick_q, ordered).astype(BF)
    qb[m] = q_ref[...]
    zrow = pl.multiple_of(z * zb, 16)
    zrx[pl.ds(zrow, zb), :] = og_ref[pl.ds(zrow, zb), :]
    pl.semaphore_wait(bar, len(peers))

    for k in sorted(range(1, nz), key=lambda d: -min(d, nz - d)):
        to = pl.multiple_of(zz(k) * zb, 16)
        send(og_ref.at[pl.ds(to, zb)], zrx.at[pl.ds(zrow, zb)], zs.at[k], zr.at[k], dz=zz(k))
    for k in range(1, nx):
        send(kv_ref, kvb.at[z, x], kxs.at[k], kxr.at[k], dx=xx(k))
    send(q_ref, qb.at[m], qs.at[0], qr.at[0], dc=oc)
    send(q_ref, qb.at[m], qs.at[1], qr.at[1], dy=ysw)
    send(q_ref, qb.at[m], qs.at[2], qr.at[2], dy=ysw, dc=oc)

    lwo.wait()
    for k in (1, 7, 2, 6, 3, 5, 4):
        send(wall.at[x, c, y], wall.at[x, c, y], wys.at[k], wyr.at[k], dy=yy(k))

    def spread(k):
        g = wall.at[x, c, yy(-k)]
        if k:
            rc(g, g, wys.at[k], wyr.at[k]).wait_recv()
        for j in range(1, nx):
            send(g, g, wxs.at[k, j], wxr.at[k, j], dx=xx(j))

    spread(0)

    for j in range(8):
        qd[j] = jnp.zeros((128, 512), BF)
        acc[j] = jnp.zeros((ODIM, 256), F32)

    def ring(step, i):
        if step < nz // 2:
            g = kvb.at[zz(-step), xx(i)]
            send(g, g, rrs.at[step, i], rrr.at[step, i], dz=zz(1))
        if step < (nz - 1) // 2:
            g = kvb.at[zz(step), xx(i)]
            send(g, g, rls.at[step, i], rlr.at[step, i], dz=zz(-1))

    def ring_wait(step):
        got = []
        if step < nz // 2:
            got.append(zz(-step - 1))
        if step < (nz - 1) // 2:
            got.append(zz(step + 1))
        for i in range(nx):
            if step < nz // 2:
                g = kvb.at[zz(-step - 1), xx(i)]
                rc(g, g, rrs.at[step, i], rrr.at[step, i]).wait_recv()
            if step < (nz - 1) // 2:
                g = kvb.at[zz(step + 1), xx(i)]
                rc(g, g, rls.at[step, i], rlr.at[step, i]).wait_recv()
            ring(step + 1, i)
        return got

    for k in range(1, nz):
        frm = pl.multiple_of(zz(-k) * zb, 16)
        rc(og_ref.at[pl.ds(0, zb)], zrx.at[pl.ds(frm, zb)], zs.at[k], zr.at[k]).wait_recv()
    xsb[...] = dot_t(pb_ref[...], zrx[...]).astype(BF)
    cl = pl.multiple_of(c * 128, 128)
    ocl = pl.multiple_of(oc * 128, 128)
    xrow = pl.multiple_of(x * xbk, 16)
    slots = (yy(0), yy(4))
    for i in range(2):
        xb[slots[i], pl.ds(xrow, xbk), pl.ds(cl, 128)] = xsb[pl.ds(xrow, xbk), i * 128 : (i + 1) * 128]
    for k in sorted(range(1, nx), key=lambda d: -min(d, nx - d)):
        to = pl.multiple_of(xx(k) * xbk, 16)
        for i in range(2):
            send(
                xsb.at[pl.ds(to, xbk), pl.ds(i * 128, 128)],
                xb.at[slots[i], pl.ds(xrow, xbk), pl.ds(cl, 128)],
                xs.at[i, k], xr.at[i, k], dx=xx(k),
            )

    ring(0, 0)
    for k in range(1, nx):
        rc(kv_ref, kvb.at[z, xx(-k)], kxs.at[k], kxr.at[k]).wait_recv()
        ring(0, nx - k)

    rc(q_ref, qb.at[b * 2 + oc], qs.at[0], qr.at[0]).wait_recv()
    rc(q_ref, qb.at[(1 - b) * 2 + c], qs.at[1], qr.at[1]).wait_recv()
    rc(q_ref, qb.at[(1 - b) * 2 + oc], qs.at[2], qr.at[2]).wait_recv()
    for mt in range(4):
        for rp in range(2):
            pair = [qb[2 * rp + i, :, mt * 128 : (mt + 1) * 128] for i in range(2)]
            pair = jnp.concatenate(pair, axis=1)
            qd[mt * 2 + rp, 0:64, 0:256] = pair
            qd[mt * 2 + rp, 64:128, 256:512] = pair

    def attend(zi):
        keys = kvb[zi, :, 0:64, :].reshape(nx * 64, 128)
        vals = [kvb[zi, i, 64:128, :] for i in range(nx)]
        vals = jnp.concatenate(vals, axis=1)
        vals = jnp.concatenate([vals, jnp.ones((ODIM - 64, nx * 128), BF)], axis=0)

        def project(p):
            parts = []
            for i in range(nx):
                parts.append(p[i * 64 : (i + 1) * 64, 0:256])
                parts.append(p[i * 64 : (i + 1) * 64, 256:512])
            return jnp.concatenate(parts, axis=0)

        scores = [dot(keys, qd[0]), dot(keys, qd[1])]
        held = None
        for j in range(8):
            p = project(jnp.exp(scores[j]).astype(BF))
            if j < 6:
                scores.append(dot(keys, qd[j + 2]))
            if held is not None:
                acc[j - 1] += dot(vals, held)
            held = p
        acc[7] += dot(vals, held)

    for k in (1, 7, 2, 6):
        spread(k)
    attend(z)

    for k in range(1, nx):
        frm = pl.multiple_of(xx(-k) * xbk, 16)
        for i in range(2):
            rc(
                xsb.at[pl.ds(0, xbk), pl.ds(i * 128, 128)],
                xb.at[slots[i], pl.ds(frm, xbk), pl.ds(cl, 128)],
                xs.at[i, k], xr.at[i, k],
            ).wait_recv()

    def half(slot, which):
        return xb.at[slot, :, pl.ds(which, 128)]

    plan = ((1, 0), (1, 4), (-1, 0), (-1, 4), (2, 0), (-2, 0))
    for i, (k, r) in enumerate(plan):
        g = half(yy(r), cl)
        send(g, g, ys.at[i], yr.at[i], dy=yy(k))

    def swap(r):
        g = half(yy(r), cl)
        send(g, g, ds.at[r], dr.at[r], dc=oc)

    swap(0)
    swap(4)
    for k in (3, 5, 4):
        spread(k)
    send(wall.at[x, c], wall.at[x, c], wds.at[0], wdr.at[0], dc=oc)

    def arrive(i):
        k, r = plan[i]
        g = half(yy(r - k), cl)
        rc(g, g, ys.at[i], yr.at[i]).wait_recv()
        swap((r - k + NY) % NY)

    steps = max(nz // 2, (nz - 1) // 2)
    for step in range(max(steps - 2, 0)):
        for zi in ring_wait(step):
            attend(zi)
    def first_layer(r, fresh):
        s = yy(r)
        g = half(s, ocl)
        rc(g, g, ds.at[r], dr.at[r]).wait_recv()
        w0 = pl.multiple_of(s * 256, 256)
        gd = dot(xb[s], wg[pl.ds(w0, 256), :])
        ud = dot(xb[s], wu[pl.ds(w0, 256), :])
        if fresh:
            ga[...] = gd
            up[...] = ud
        else:
            ga[...] += gd
            up[...] += ud

    lwg.wait()
    lwu.wait()
    first_layer(0, True)
    first_layer(4, False)
    coming = (0, 2, 1, 3, 4, 5)
    for n, i in enumerate(coming):
        arrive(i)
        if n >= 1:
            k, r = plan[coming[n - 1]]
            first_layer((r - k + NY) % NY, False)
    later = ring_wait(steps - 2) if steps > 1 else []
    k, r = plan[coming[5]]
    first_layer((r - k + NY) % NY, False)
    gate = ga[...]
    hid = (gate / (1.0 + jnp.exp(-gate)) * up[...]).astype(BF)
    for copy in lwd:
        copy.wait()
    def paired(r):
        rc(pbuf.at[r], prx.at[r], es.at[r], er.at[r]).wait_recv()
        return own[r] + prx[r].astype(F32)

    order = (4, 3, 5, 1, 7, 2, 6, 0)
    route = {4: (0, yy(0 - 2 * sgn)), 3: (1, yy(1)), 5: (2, yy(-1)), 1: (3, yy(1)), 7: (4, yy(-1))}
    for n in range(8 + 2):
        if n < 8:
            r = order[n]
            tmp[r % 2] = dot(hid, wd[yy(r)])
            own[r] = tmp[r % 2, :, pl.ds(cl, 128)]
            pbuf[r] = tmp[r % 2, :, pl.ds(ocl, 128)].astype(BF)
            send(pbuf.at[r], prx.at[r], es.at[r], er.at[r], dc=oc)
        if n >= 2 and order[n - 2] in route:
            r = order[n - 2]
            i, dest = route[r]
            psb[r] = paired(r).astype(BF)
            send(psb.at[r], rs.at[i], ms.at[i], mr.at[i], dy=dest)

    def got_rs(i):
        rc(psb.at[0], rs.at[i], ms.at[i], mr.at[i]).wait_recv()
        return rs[i].astype(F32)

    for zi in later:
        attend(zi)
    far_sum = got_rs(0)
    right = c.astype(F32)
    psb[2] = (paired(2) + got_rs(1) + far_sum * right).astype(BF)
    send(psb.at[2], rs.at[5], ms.at[5], mr.at[5], dy=yy(2))
    psb[6] = (paired(6) + got_rs(2) + far_sum * (1.0 - right)).astype(BF)
    send(psb.at[6], rs.at[6], ms.at[6], mr.at[6], dy=yy(-2))

    for zi in ring_wait(steps - 1):
        attend(zi)
    for j in range(8):
        a = acc[j]
        den = a[64:ODIM]
        hi = den.astype(BF)
        lo = (den - hi.astype(F32)).astype(BF)
        first = lax.broadcasted_iota(jnp.int32, (ODIM - 64, 256), 0) == 0
        ob[j, 0:64] = a[0:64].astype(BF)
        ob[j, 64:ODIM] = jnp.where(first, hi.astype(F32), lo.astype(F32)).astype(BF)
    members = ((0, y, oc, b * 2 + oc), (1, ysw, c, (1 - b) * 2 + c), (2, ysw, oc, (1 - b) * 2 + oc))
    for i, dy, dc, mm in members:
        send(ob.at[pl.ds(2 * mm, 2)], orx.at[i], ts.at[i], tr.at[i], dy=dy, dc=dc)

    ret[...] = (paired(0) + got_rs(3) + got_rs(4) + got_rs(5) + got_rs(6)).astype(BF)
    rbk[pl.ds(xrow, xbk), :] = ret[pl.ds(xrow, xbk), :]
    for k in sorted(range(1, nx), key=lambda d: -min(d, nx - d)):
        to = pl.multiple_of(xx(k) * xbk, 16)
        send(ret.at[pl.ds(to, xbk)], rbk.at[pl.ds(xrow, xbk)], vs.at[k], vr.at[k], dx=xx(k))
    for k in range(1, nx):
        for j in range(NY):
            g = wall.at[xx(-k), c, yy(-j)]
            rc(g, g, wxs.at[j, k], wxr.at[j, k]).wait_recv()
        g = wall.at[xx(-k), c]
        send(g, g, wds.at[k], wdr.at[k], dc=oc)
    for i, dy, dc, mm in members:
        rc(ob.at[pl.ds(0, 2)], orx.at[i], ts.at[i], tr.at[i]).wait_recv()
    heads = []
    for rp in range(2):
        t = ob[2 * m + rp].astype(F32)
        for i in range(3):
            t += orx[i, rp].astype(F32)
        o = (t[0:64] / (t[64:65] + t[65:66])).astype(BF)
        heads += [o[:, 0:128], o[:, 128:256]]
    heads = jnp.concatenate(heads, axis=0)
    square = (iota((256, 256), 0) == iota((256, 256), 1)).astype(F32).astype(BF)
    ho[...] = dot_t(heads, square).astype(BF).reshape(4, 32, 256)
    hb[h] = ho[h]
    for k in range(1, 4):
        send(ho.at[lax.rem(h + k, 4)], hb.at[h], as_.at[k - 1], ar.at[k - 1], dy=yy(2 * k))

    for k in range(1, nx):
        frm = pl.multiple_of(xx(-k) * xbk, 16)
        rc(ret.at[pl.ds(0, xbk)], rbk.at[pl.ds(frm, xbk)], vs.at[k], vr.at[k]).wait_recv()
    t2[...] = dot(pb_ref[...], rbk[...]).astype(BF)
    fin[pl.ds(zrow, zb), :] = t2[pl.ds(zrow, zb), :]
    for k in sorted(range(1, nz), key=lambda d: -min(d, nz - d)):
        to = pl.multiple_of(zz(k) * zb, 16)
        send(t2.at[pl.ds(to, zb)], fin.at[pl.ds(zrow, zb)], us.at[k], ur.at[k], dz=zz(k))

    for k in range(1, nx):
        g = wall.at[xx(-k), oc]
        rc(g, g, wds.at[k], wdr.at[k]).wait_recv()
    rc(wall.at[x, oc], wall.at[x, oc], wds.at[0], wdr.at[0]).wait_recv()
    for k in range(1, 4):
        rc(ho.at[0], hb.at[lax.rem(h - k + 4, 4)], as_.at[k - 1], ar.at[k - 1]).wait_recv()
    columns = []
    for n in range(nx):
        part = None
        for g in range(4):
            w = jnp.concatenate([wall[n, r % 2, 2 * g + r // 2] for r in range(4)], axis=0)
            part = dot(hb[g], w) if part is None else part + dot(hb[g], w)
        columns.append(part)
    mixed = jnp.concatenate(columns, axis=1)
    scale = lax.rsqrt(jnp.mean(mixed * mixed, axis=1, keepdims=True) + EPSILON)
    lpost.wait()
    out_ref[...] = (mixed * scale * pg_ref[...]).astype(BF)

    logits = lg_ref[...]
    grown = jnp.exp(logits - jnp.max(logits, axis=0, keepdims=True))
    weight = lax.dot_general(
        eye, grown / jnp.sum(grown, axis=0, keepdims=True), (((1,), (1,)), ((), ())),
        precision=lax.Precision.HIGHEST, preferred_element_type=F32,
    )

    for k in range(1, nz):
        frm = pl.multiple_of(zz(-k) * zb, 16)
        rc(t2.at[pl.ds(0, zb)], fin.at[pl.ds(frm, zb)], us.at[k], ur.at[k]).wait_recv()
    total = weight[:, 0:1] * dot(pick[0].astype(F32).astype(BF), fin[...])
    total += weight[:, 1:2] * dot(pick[1].astype(F32).astype(BF), fin[...])
    moe_ref[...] = total.astype(BF)
    for copy in sent:
        copy.wait_send()


def call(nz, nx, cap, *args):
    rows = nz * nx * cap
    vm = pl.BlockSpec(memory_space=pltpu.VMEM)
    hbm = pl.BlockSpec(memory_space=pltpu.HBM)
    dma = lambda *n: pltpu.SemaphoreType.DMA(n)
    big = lambda *s: pltpu.VMEM(s, BF)
    wide = lambda *s: pltpu.VMEM(s, F32)
    scratch = [
        big(64, 512), big(128, 128), big(128, 128), big(128, 2048), wide(1, 2048), wide(1, 2048),
        big(64, 512), big(128, 128), big(rows, 256), big(rows, rows),
        big(nz, nx, 128, 128), big(4, 64, 512), big(8, 128, 512), wide(8, ODIM, 256), big(8, ODIM, 256),
        big(3, 2, ODIM, 256), big(nx, 2, NY, 64, 2048 // nx), big(4, 32, 256), big(4, 32, 256),
        big(rows, 256), big(rows, 256), big(NY, rows, 256), big(2048, 256), big(2048, 256), big(NY, 256, 256),
        wide(rows, 256), wide(rows, 256), wide(2, rows, 256), wide(NY, rows, 128), big(NY, rows, 128),
        big(NY, rows, 128), big(NY, rows, 128), big(7, rows, 128), big(rows, 128), big(rows, 128),
        big(rows, 128), big(rows, 128),
        dma(17), dma(nx), dma(nx), dma(nz, nx), dma(nz, nx), dma(nz, nx), dma(nz, nx), dma(3), dma(3), dma(3), dma(3), dma(NY), dma(NY), dma(NY, nx), dma(NY, nx),
        dma(nx), dma(nx), dma(3), dma(3),
        dma(nz), dma(nz), dma(2, nx), dma(2, nx), dma(6), dma(6), dma(8), dma(8), dma(8), dma(8), dma(7), dma(7),
        dma(nx), dma(nx), dma(nz), dma(nz),
    ]
    return pl.pallas_call(
        functools.partial(kernel, nz, nx, cap),
        out_shape=(jax.ShapeDtypeStruct((32, 2048), BF), jax.ShapeDtypeStruct((128, 128), BF)),
        in_specs=[vm] * 6 + [hbm] * 10,
        out_specs=(vm, vm),
        scratch_shapes=scratch,
        compiler_params=pltpu.CompilerParams(
            collective_id=0, has_side_effects=True, vmem_limit_bytes=67043328 - 200 * 1024
        ),
        name="layer",
    )(*args)


def per_device(
    q_in, k_in, v_in, q_gain, k_gain, w_out, post_gain, moe_in, routes, route_logits, pre_gain, w_gate, w_up, w_down
):
    nz, nx = lax.axis_size("z"), lax.axis_size("x")
    count, top = routes.shape
    experts = nz * nx
    cap = max(2, 3 * top * count // (2 * experts))
    i = np.arange(experts * cap, dtype=np.int32)
    src = (i % (nz * cap)) // cap * (nx * cap) + i // (nz * cap) * cap + i % cap
    return call(
        nz, nx, cap, jnp.asarray(angle_table()), q_gain[None, :], k_gain[None, :], routes.T, route_logits.T,
        jnp.asarray(src[None, :]), pre_gain[None, :], post_gain[None, :],
        q_in.T, k_in, v_in, moe_in, w_gate[0], w_up[0], w_down[0], w_out,
    )


def solution(mesh):
    ny = mesh.shape["tp"] // 2
    nz = 8 if mesh.shape["ep"] % 8 == 0 else 2
    finer = Mesh(mesh.devices.reshape(nz, mesh.shape["ep"] // nz, ny, 2), ALL)
    in_specs = (
        P(EP, TP), P(EP, None), P(EP, None), P(), P(), P(TP, None), P(), P(EP, None), P(EP, None), P(EP, None), P(),
        P(EP, None, TP), P(EP, None, TP), P(EP, TP, None),
    )
    return jax.shard_map(
        per_device, mesh=finer, in_specs=in_specs, out_specs=(P(ALL, None), P(EP, TP)), check_vma=False
    )
```
